32 devices in a mesh: sp: 8 (over z, y), tp: 4 (over x, core).
Axes of the slice: x: 2, y: 2, z: 4, core: 2. Of those that a mesh axis runs over, the one named last changes fastest.
Arguments:
- out_grad: bfloat16 [2048, 4096], P('sp'), may hold values from -6 to 6
- stream: bfloat16 [2048, 4096], P('sp'), may hold values from -6 to 6
- norm_gain: bfloat16 [4096], replicated, may hold values from 0.099609375 to 1.8984375
- routes: int32 [2048, 2], P('sp'), may hold values from 0 to 7, all different within a row; in each aligned block of 256 rows (0 to 255, 256 to 511, ...) at most 80 rows name the same one
- route_weight: float32 [2048, 2], P('sp'), may hold values from 0.3 to 1.5
- gate_weight: bfloat16 [8, 4096, 1024], P('sp', None, 'tp'), may hold values from -0.09375 to 0.09375
- up_weight: bfloat16 [8, 4096, 1024], P('sp', None, 'tp'), may hold values from -0.09375 to 0.09375
- down_weight: bfloat16 [8, 1024, 4096], P('sp', 'tp'), may hold values from -0.1875 to 0.1875
- out_proj: bfloat16 [4096, 1024], P(None, 'tp'), may hold values from -0.1875 to 0.1875
- conv_out: bfloat16 [2048, 1024], P('sp', 'tp'), as said below
- gate_branch: bfloat16 [2048, 1024], P('sp', 'tp'), may hold values from -6 to 6
- decay_map: bfloat16 [2, 4, 256, 256], P(None, 'tp'), as said below
- input_map: bfloat16 [2, 4, 256, 256], P(None, 'tp'), as said below
- decay_param: float32 [2, 1024], P(None, 'tp'), as said below
- decay_shift: float32 [2, 2048, 1024], P(None, 'sp', 'tp'), as said below
- states: float32 [2, 2048, 1024], P(None, 'sp', 'tp'), as said below
Outputs:
- conv_grad: float32 [2048, 1024], P('sp', 'tp')
- gate_branch_grad: float32 [2048, 1024], P('sp', 'tp')
- out_proj_grad: float32 [4096, 1024], P('sp', 'tp')
- gate_weight_grad: bfloat16 [8, 4096, 1024], P('sp', None, 'tp')
- up_weight_grad: bfloat16 [8, 4096, 1024], P('sp', None, 'tp')
- down_weight_grad: bfloat16 [8, 1024, 4096], P('sp', 'tp')
The draws below stay inside these ranges and needn't reach their ends.
Inputs may be any that keep to these rules, and one draw needn't show every extreme that they name: `routes`: each token names 2 different experts. Among the 256 tokens of one index of sp no expert is named more than 80 times, a bound that some expert reaches in some of these blocks. `conv_out`: within -6 to 6. `decay_map`: entries within -4 to 4 times 256 to the power -0.5. `input_map`: entries within -4 to 4 times 256 to the power -0.5. `decay_param`: between 3.7 and 3.5 plus the logarithm of 2048. `decay_shift`: every entry lies between -0.7 and -0.00002. The forward pass's states: they follow the recurrences of the steps from conv_out, decay_map, input_map, decay_param and decay_shift.
All inputs are finite; a program needn't handle non-finite values.
Results may differ from the reference program's by a relative error of at most 0.018.
Values may be sent and summed in bfloat16 or wider, within the bound.
A program may use at most 128 MiB of HBM per device.

```python
import math
import jax
import jax.numpy as jnp
import numpy as np
from jax import lax

D = 4096
RECURRENT_WIDTH = 1024
BLOCKS = 4
BW = 256
FF = 1024
TOP = 2
TOK_DEV = 256
EXPERTS = 8
SEQUENCE_TOKENS = 2048
CAP = 80
N_SP = 8
N_TP = 4


def scan_pairs(coeffs, values, reverse):

    def combine(earlier, later):
        return (earlier[0] * later[0], later[0] * earlier[1] + later[1])
    return lax.associative_scan(combine, (coeffs, values), axis=0, reverse=reverse)[1]


def block_apply(channels, block_maps):
    shaped = channels.reshape(channels.shape[0], block_maps.shape[0], block_maps.shape[1])
    mapped = jnp.einsum('tkc,kcd->tkd', shaped, block_maps.astype(jnp.float32), precision=lax.Precision.HIGHEST)
    return mapped.reshape(channels.shape)


def lru_draw(key):
    random_keys = jax.random.split(jax.random.fold_in(key, 4242), 9)
    conv_field = jax.random.normal(random_keys[1], (SEQUENCE_TOKENS, RECURRENT_WIDTH), jnp.float32)
    fast_share = 0.5
    conv_field = jnp.clip(conv_field, -6.0, 6.0).astype(jnp.bfloat16)
    gate_maps = jnp.clip(jax.random.normal(random_keys[2], (2, 2, BLOCKS, BW, BW), jnp.float32), -4.0, 4.0)
    gate_maps = (gate_maps * BW ** (-0.5)).astype(jnp.bfloat16)
    fast_mask = jax.random.uniform(random_keys[3], (2, RECURRENT_WIDTH), jnp.float32) < fast_share
    slow_values = jnp.log(SEQUENCE_TOKENS * 1.0) + jax.random.uniform(random_keys[4], (2, RECURRENT_WIDTH), jnp.float32, 2.0, 3.5)
    fast_values = jax.random.uniform(random_keys[5], (2, RECURRENT_WIDTH), jnp.float32, 3.7, 4.9)
    decay_values = jnp.where(fast_mask, fast_values, slow_values)
    block_count = SEQUENCE_TOKENS // TOK_DEV
    block_rate = jnp.exp(jax.random.uniform(random_keys[6], (2, block_count), jnp.float32, -10.6, -9.2))
    shift_offset = -jnp.repeat(block_rate, TOK_DEV, axis=1)[:, :, None]
    spike_mask = jax.random.uniform(random_keys[7], (2, SEQUENCE_TOKENS, RECURRENT_WIDTH), jnp.float32) < 1.5 / SEQUENCE_TOKENS
    spike_depth = jnp.log(jax.random.uniform(random_keys[8], (2, SEQUENCE_TOKENS, RECURRENT_WIDTH), jnp.float32, 0.5, 0.8))
    offset_field = shift_offset + jnp.where(spike_mask, spike_depth, 0.0)
    conv_float = conv_field.astype(jnp.float32)
    state_list = []
    for direction in range(2):
        decay_gate = jax.nn.sigmoid(block_apply(conv_float, gate_maps[0, direction]))
        input_gate = jax.nn.sigmoid(block_apply(conv_float, gate_maps[1, direction]))
        log_decay = -8.0 * decay_gate * jax.nn.softplus(-decay_values[direction])[None, :] + offset_field[direction]
        drive_term = jnp.sqrt(-jnp.expm1(2.0 * log_decay)) * input_gate * conv_float
        state_list.append(scan_pairs(jnp.exp(log_decay), drive_term, direction == 1))
    return (conv_field, gate_maps[0], gate_maps[1], decay_values, offset_field, jnp.stack(state_list))


def draw_conv_out(key, part):
    return lru_draw(key)[0]


def draw_decay_map(key, part):
    return lru_draw(key)[1]


def draw_input_map(key, part):
    return lru_draw(key)[2]


def draw_decay_param(key, part):
    return lru_draw(key)[3]


def draw_decay_shift(key, part):
    return lru_draw(key)[4]


def draw_states(key, part):
    return lru_draw(key)[5]


def raised(values, rng, source, target, blocks, factor):
    owner, partner = [(jnp.arange(values.shape[position]) // (values.shape[position] // blocks)).reshape([-1 if axis == position else 1 for axis in range(values.ndim)]) for position in (source, target)]
    chosen = jax.random.permutation(rng, blocks)[partner]
    strong = (owner == chosen) | (owner == (partner + blocks // 2) % blocks)
    return jnp.where(strong, factor * values, values)


def levels(key, dims, pieces, least, largest):
    loudness = 1.0
    for position, parts in pieces:
        heights = jax.random.uniform(jax.random.fold_in(jax.random.fold_in(key, 6), position), (parts,), jnp.float32, least / len(pieces), largest / len(pieces))
        loudness = loudness * jnp.repeat(jnp.exp(heights), dims[position] // parts).reshape((-1,) + (1,) * (len(dims) - 1 - position))
    return loudness


def deal_out(key, own, number, rows, number_of, top, most, lean):
    order = jax.random.permutation(key, number_of)
    crowded, common = load_shares(number_of, rows * top, most, lean, True), load_shares(number_of, rows * top, most, lean, False)
    places = jnp.arange(number_of)

    def named(tallies, offset_by):
        used = int((tallies > 0).sum())
        fixed = max(1, used // 4)
        shifted = fixed + (places - fixed + offset_by * (used - fixed)) % max(1, number_of - fixed)
        return jnp.zeros((number_of,), jnp.int32).at[order[jnp.where(places < fixed, places, shifted)]].set(jnp.asarray(tallies, jnp.int32))

    tallies = jnp.where(number % 4 == 0, named(crowded, number // 4), named(common, number - number // 4 - 1))
    mixed = jax.random.permutation(jax.random.fold_in(own, 3), number_of)
    donor, sink = mixed[0:number_of // 2 * 2:2], mixed[1:number_of // 2 * 2:2]
    room = jnp.minimum(tallies[donor] - 1, most - tallies[sink]) // 2
    room = jnp.where((donor == order[0]) | (sink == order[0]) | (tallies[sink] == 0), 0, jnp.maximum(room, 0))
    shifted = jax.random.randint(jax.random.fold_in(own, 4), (number_of // 2,), 0, 1 << 20) % (room + 1)
    tallies = tallies.at[donor].add(-shifted).at[sink].add(shifted)
    members = jnp.searchsorted(jnp.cumsum(tallies), jnp.arange(rows * top), side="right").astype(jnp.int32)
    grid = members.reshape(top, rows).T
    grid = grid[jax.random.permutation(jax.random.fold_in(own, 1), rows)]
    offset_by = jax.random.randint(jax.random.fold_in(own, 2), (rows, 1), 0, top)
    return jnp.take_along_axis(grid, (jnp.arange(top)[None, :] + offset_by) % top, axis=1)


def load_shares(count, total, limit, skew, full):
    loads = [(1 << 20) // math.isqrt(standing ** skew) + 1 for standing in range(1, count + 1)]
    largest = limit if full else min(limit, max(-(-total // count), total * loads[0] // sum(loads)))
    least = 1 if total - largest >= count - 1 else 0
    counts, rest = [largest] + [least] * (count - 1), total - largest - least * (count - 1)
    while rest > 0:
        movable = [i for i in range(1, count) if counts[i] < largest] or [i for i in range(1, count) if counts[i] < limit]
        whole, remaining = sum([loads[i] for i in movable]), rest
        for i in movable:
            more = min(limit - counts[i], max(1, remaining * loads[i] // whole), rest)
            counts[i] = counts[i] + more
            rest = rest - more
    return np.array(counts)


def bell_draw(stream_key, shape, deviation, reach, shards=(), held_as=jnp.bfloat16):
    drawn = deviation * jax.random.normal(stream_key, shape, jnp.float32)
    if shards:
        drawn = drawn * levels(stream_key, shape, shards, -0.22, 0.18)
    return jnp.clip(drawn, -reach, reach).astype(held_as)


def noise_with(own_key, dims, deviation, most, cuts, heavy, kind=jnp.bfloat16):
    array = deviation * jax.random.normal(own_key, dims, jnp.float32)
    if cuts:
        array = array * levels(own_key, dims, cuts, -0.22, 0.18)
    return jnp.clip(raised(array, jax.random.fold_in(own_key, 3), *heavy), -most, most).astype(kind)


def setup_inputs(seed: int = 0) -> dict:
    key_of = jax.random.split(jax.random.key(seed), 17)
    out_grad = noise_with(key_of[0], (SEQUENCE_TOKENS, D), 1.0, 6.0, ((0, 8),), (0, 1, 8, 2.0))
    stream = bell_draw(key_of[1], (SEQUENCE_TOKENS, D), 1.0, 6.0, ((0, 8),))
    norm_gain = jnp.clip(1.0 + 0.18 * jax.random.normal(key_of[2], (D,), jnp.float32), 0.099609375, 1.8984375).astype(jnp.bfloat16)
    routes_keys = jax.random.split(jax.random.fold_in(key_of[3], 1), SEQUENCE_TOKENS // TOK_DEV)
    routes_turns = jax.random.permutation(jax.random.fold_in(key_of[3], 3), SEQUENCE_TOKENS // TOK_DEV)
    routes = jax.vmap(lambda own, number: deal_out(jax.random.fold_in(key_of[3], 2), own, number, TOK_DEV, EXPERTS, TOP, CAP, 1))(routes_keys, routes_turns).reshape((SEQUENCE_TOKENS, TOP))
    route_weight = jnp.clip(0.3 + 1.2 * jax.random.uniform(key_of[4], (SEQUENCE_TOKENS, TOP), jnp.float32) ** levels(key_of[4], (SEQUENCE_TOKENS, TOP), ((0, 8),), -0.2, 0.2), 0.3, 1.5)
    gate_weight = bell_draw(key_of[5], (EXPERTS, D, FF), D ** -0.5, 0.09375, ((0, 8), (2, 4)))
    up_weight = bell_draw(key_of[6], (EXPERTS, D, FF), D ** -0.5, 0.09375, ((0, 8), (2, 4)))
    down_weight = bell_draw(key_of[7], (EXPERTS, FF, D), FF ** -0.5, 0.1875, ((0, 8), (1, 4)))
    out_proj = bell_draw(key_of[8], (D, RECURRENT_WIDTH), RECURRENT_WIDTH ** -0.5, 0.1875, ((1, 4),))
    conv_out = draw_conv_out(jax.random.fold_in(key_of[16], 71), 0)
    gate_branch = bell_draw(key_of[10], (SEQUENCE_TOKENS, RECURRENT_WIDTH), 1.0, 6.0, ((0, 8), (1, 4)))
    decay_map = draw_decay_map(jax.random.fold_in(key_of[16], 71), 0)
    input_map = draw_input_map(jax.random.fold_in(key_of[16], 71), 0)
    decay_param = draw_decay_param(jax.random.fold_in(key_of[16], 71), 0)
    decay_shift = draw_decay_shift(jax.random.fold_in(key_of[16], 71), 0)
    states = draw_states(jax.random.fold_in(key_of[16], 71), 0)
    return dict(out_grad=out_grad, stream=stream, norm_gain=norm_gain, routes=routes, route_weight=route_weight, gate_weight=gate_weight, up_weight=up_weight, down_weight=down_weight, out_proj=out_proj, conv_out=conv_out, gate_branch=gate_branch, decay_map=decay_map, input_map=input_map, decay_param=decay_param, decay_shift=decay_shift, states=states)


rate_scale = 8.0
norm_eps = 1e-06

def contract(left, right, left_dim, right_dim):
    return lax.dot_general(left, right, (((left_dim,), (right_dim,)), ((), ())), preferred_element_type=jnp.float32)

def linear_scan(coeffs, values, reverse):

    def combine(earlier, later):
        return (earlier[0] * later[0], later[0] * earlier[1] + later[1])
    return lax.associative_scan(combine, (coeffs, values), axis=0, reverse=reverse)

def silu_grad(values):
    logistic = jax.nn.sigmoid(values)
    return logistic * (1.0 + values * (1.0 - logistic))

def expert_pass(slot_inputs, slot_cotan, gate_local, up_local, down_local):
    gate_pre = contract(slot_inputs, gate_local, 1, 0)
    up_pre = contract(slot_inputs, up_local, 1, 0)
    hidden = (jax.nn.silu(gate_pre) * up_pre).astype(jnp.bfloat16)
    down_wgrad = contract(hidden, slot_cotan, 0, 0)
    hidden_grad = contract(slot_cotan, down_local, 1, 1)
    up_grad = (hidden_grad * jax.nn.silu(gate_pre)).astype(jnp.bfloat16)
    gate_grad = (hidden_grad * up_pre * silu_grad(gate_pre)).astype(jnp.bfloat16)
    gate_wgrad = contract(slot_inputs, gate_grad, 0, 0)
    up_wgrad = contract(slot_inputs, up_grad, 0, 0)
    return (gate_wgrad, up_wgrad, down_wgrad, gate_grad, up_grad)

def block_forward(channels, block_maps):
    shaped = channels.reshape(channels.shape[0], block_maps.shape[0], block_maps.shape[1])
    mapped = jnp.einsum('tkc,kcd->tkd', shaped, block_maps.astype(jnp.float32), precision=lax.Precision.HIGHEST)
    return mapped.reshape(channels.shape)

def block_backward(pre_grad, block_maps):
    shaped = pre_grad.reshape(pre_grad.shape[0], block_maps.shape[0], block_maps.shape[2])
    mapped = jnp.einsum('tkd,kcd->tkc', shaped, block_maps.astype(jnp.float32), precision=lax.Precision.HIGHEST)
    return mapped.reshape(pre_grad.shape)

def recurrence_back(adjoint, state_run, conv_float, gate_parts, decay_local, input_local):
    decay_gate, input_gate, decay_base, decay_rate, drive_scale, drive_term = gate_parts
    log_grad = adjoint * (state_run - drive_term) - adjoint * input_gate * conv_float * decay_rate * decay_rate / drive_scale
    decay_pre_grad = log_grad * (-rate_scale * decay_base) * decay_gate * (1.0 - decay_gate)
    input_pre_grad = adjoint * drive_scale * conv_float * input_gate * (1.0 - input_gate)
    return adjoint * drive_scale * input_gate + block_backward(decay_pre_grad, decay_local) + block_backward(input_pre_grad, input_local)

def reference(out_grad, stream, norm_gain, routes, route_weight, gate_weight, up_weight, down_weight, out_proj, conv_out, gate_branch, decay_map, input_map, decay_param, decay_shift, states):
    stream_f = stream.astype(jnp.float32)
    row_scale = lax.rsqrt(lax.optimization_barrier(jnp.mean(stream_f * stream_f, axis=1, keepdims=True)) + norm_eps)
    unit_rows = stream_f * row_scale
    gain_row = norm_gain.astype(jnp.float32)[None, :]
    normed = (unit_rows * gain_row).astype(jnp.bfloat16)
    pair_count = SEQUENCE_TOKENS * TOP
    pair_expert = routes.reshape(N_SP, TOK_DEV * TOP)
    onehot = (pair_expert[:, :, None] == jnp.arange(EXPERTS, dtype=jnp.int32)[None, None, :]).astype(jnp.int32)
    slot_rank = lax.optimization_barrier(jnp.sum((jnp.cumsum(onehot, axis=1) - onehot) * onehot, axis=2))
    source = jnp.arange(N_SP, dtype=jnp.int32)[:, None]
    slot_index = (pair_expert * (N_SP * CAP) + source * CAP + slot_rank).reshape(-1).astype(jnp.int32)
    slot_pair = jnp.full((EXPERTS * N_SP * CAP,), pair_count, jnp.int32).at[slot_index].set(jnp.arange(pair_count, dtype=jnp.int32))
    slot_token = (slot_pair // TOP).astype(jnp.int32)
    zero_row = jnp.zeros((1, D), jnp.bfloat16)
    slot_inputs = jnp.concatenate([normed, zero_row])[slot_token].reshape(EXPERTS, N_SP * CAP, D)
    weight_pad = jnp.concatenate([route_weight.reshape(-1), jnp.zeros((1,), jnp.float32)])
    slot_cotan = (weight_pad[slot_pair][:, None] * jnp.concatenate([out_grad, zero_row])[slot_token].astype(jnp.float32)).astype(jnp.bfloat16)
    slot_cotan = slot_cotan.reshape(EXPERTS, N_SP * CAP, D)

    def one_expert(operands):
        inputs_e, cotan_e, gate_local, up_local, down_local = operands
        gate_wgrad, up_wgrad, down_wgrad, gate_grad, up_grad = expert_pass(inputs_e, cotan_e, gate_local, up_local, down_local)
        run_width = FF // N_TP
        total_sum = jnp.zeros((inputs_e.shape[0], D), jnp.float32)
        for quarter in range(N_TP):
            low_unit = quarter * run_width
            high_unit = low_unit + run_width
            partial_value = contract(gate_grad[:, low_unit:high_unit], gate_local[:, low_unit:high_unit], 1, 1) + contract(up_grad[:, low_unit:high_unit], up_local[:, low_unit:high_unit], 1, 1)
            total_sum = total_sum + lax.optimization_barrier(partial_value.astype(jnp.bfloat16)).astype(jnp.float32)
        return (gate_wgrad.astype(jnp.bfloat16), up_wgrad.astype(jnp.bfloat16), down_wgrad.astype(jnp.bfloat16), total_sum.astype(jnp.bfloat16))
    gate_grads, up_grads, down_grads, pair_grad = lax.map(one_expert, (slot_inputs, slot_cotan, gate_weight, up_weight, down_weight))
    returned = pair_grad.reshape(EXPERTS * N_SP * CAP, D)[slot_index]
    normed_grad = lax.optimization_barrier(jnp.sum(returned.reshape(SEQUENCE_TOKENS, TOP, D).astype(jnp.float32), axis=1))
    scaled_grad = gain_row * normed_grad
    stream_grad = out_grad.astype(jnp.float32) + row_scale * (scaled_grad - unit_rows * lax.optimization_barrier(jnp.mean(unit_rows * scaled_grad, axis=1, keepdims=True)))
    stream_grad_b = stream_grad.astype(jnp.bfloat16)
    total_state = states[0] + states[1]
    gate_float = gate_branch.astype(jnp.float32)
    gelu_gate, gelu_back = jax.vjp(jax.nn.gelu, gate_float)
    lru_out = (total_state * gelu_gate).astype(jnp.bfloat16)
    out_proj_grad = contract(stream_grad_b, lru_out, 0, 0)
    lru_out_grad = contract(stream_grad_b, out_proj, 1, 0)
    gate_branch_grad = gelu_back(lru_out_grad * total_state)[0]
    state_grad = lru_out_grad * gelu_gate
    conv_float = conv_out.astype(jnp.float32)
    ones_row = jnp.ones((1, RECURRENT_WIDTH), jnp.float32)
    conv_grad = jnp.zeros_like(conv_float)
    for direction in range(2):
        decay_gate = jax.nn.sigmoid(block_forward(conv_float, decay_map[direction]))
        input_gate = jax.nn.sigmoid(block_forward(conv_float, input_map[direction]))
        decay_base = jax.nn.softplus(-decay_param[direction])[None, :]
        log_decay = -rate_scale * decay_gate * decay_base + decay_shift[direction]
        decay_rate = jnp.exp(log_decay)
        drive_scale = jnp.sqrt(-jnp.expm1(2.0 * log_decay))
        drive_term = drive_scale * input_gate * conv_float
        if direction == 0:
            adjoint = linear_scan(jnp.concatenate([decay_rate[1:], ones_row]), state_grad, True)[1]
        else:
            adjoint = linear_scan(jnp.concatenate([ones_row, decay_rate[:-1]]), state_grad, False)[1]
        gate_parts = (decay_gate, input_gate, decay_base, decay_rate, drive_scale, drive_term)
        conv_grad = conv_grad + recurrence_back(adjoint, states[direction], conv_float, gate_parts, decay_map[direction], input_map[direction])
    return (conv_grad, gate_branch_grad, out_proj_grad, gate_grads, up_grads, down_grads)
```

```python
import functools

import jax
import jax.numpy as jnp
from jax import lax
from jax.experimental import pallas as pl
from jax.experimental.pallas import tpu as pltpu
from jax.sharding import PartitionSpec as P

TOP = 2
EXP_DEV = 1
TOK_DEV = 256


rate_scale = 8.0
norm_eps = 1e-06


def contract(left, right, left_dim, right_dim):
    return lax.dot_general(
        left, right, (((left_dim,), (right_dim,)), ((), ())), preferred_element_type=jnp.float32
    )


def silu_grad(values):
    logistic = jax.nn.sigmoid(values)
    return logistic * (1.0 + values * (1.0 - logistic))


def expert_pass(slot_inputs, slot_cotan, gate_local, up_local, down_local):
    gate_pre = contract(slot_inputs, gate_local, 1, 0)
    up_pre = contract(slot_inputs, up_local, 1, 0)
    hidden = (jax.nn.silu(gate_pre) * up_pre).astype(jnp.bfloat16)
    down_wgrad = contract(hidden, slot_cotan, 0, 0)
    hidden_grad = contract(slot_cotan, down_local, 1, 1)
    up_grad = (hidden_grad * jax.nn.silu(gate_pre)).astype(jnp.bfloat16)
    gate_grad = (hidden_grad * up_pre * silu_grad(gate_pre)).astype(jnp.bfloat16)
    gate_wgrad = contract(slot_inputs, gate_grad, 0, 0)
    up_wgrad = contract(slot_inputs, up_grad, 0, 0)
    return (gate_wgrad, up_wgrad, down_wgrad, gate_grad, up_grad)


MESH = pl.DeviceIdType.MESH


def push(source, target, send_sem, recv_sem, where):
    return pltpu.make_async_remote_copy(
        src_ref=source,
        dst_ref=target,
        send_sem=send_sem,
        recv_sem=recv_sem,
        device_id=where,
        device_id_type=MESH,
    )


def greet(sources, me, others):
    barrier = pltpu.get_barrier_semaphore()

    def one(step, carry):
        pl.semaphore_signal(
            barrier, inc=1, device_id={"sp": lax.rem(me + step, sources)}, device_id_type=MESH
        )
        return carry

    lax.fori_loop(1, sources, one, 0)
    for other in others:
        pl.semaphore_signal(barrier, inc=1, device_id={"tp": other}, device_id_type=MESH)
    pl.semaphore_wait(barrier, sources - 1 + len(others))


def loop(low, high, step):
    def one(index, carry):
        step(index)
        return carry

    lax.fori_loop(low, high, one, 0)


def quarter_at(ref, slot, quarter, width):
    return ref.at[slot, :, pl.ds(pl.multiple_of(quarter * width, width), width)]


def dispatch_kernel(
    sources, in_ref, ct_ref, oin_ref, oct_ref,
    send_a, recv_a, send_b, recv_b, send_c, recv_c, send_d, recv_d, local
):
    me, mine = lax.axis_index("sp"), lax.axis_index("tp")
    beside = mine + 1 - 2 * lax.rem(mine, 2)
    across = lax.rem(mine + 2, 4)
    diagonal = lax.rem(beside + 2, 4)
    width = in_ref.shape[2]
    pairs = ((in_ref, oin_ref), (ct_ref, oct_ref))
    owned = [
        pltpu.make_async_copy(src.at[me], quarter_at(dst, me, mine, width), local.at[arr])
        for arr, (src, dst) in enumerate(pairs)
    ]
    for copy in owned:
        copy.start()
    greet(sources, me, (beside, across))

    def first(arr, peer):
        src, dst = pairs[arr]
        return push(
            src.at[peer], quarter_at(dst, me, mine, width),
            send_a.at[arr, peer], recv_a.at[arr, me], {"sp": peer},
        )

    def first_landed(arr, origin):
        src, dst = pairs[arr]
        return push(
            src.at[me], quarter_at(dst, origin, mine, width),
            send_a.at[arr, me], recv_a.at[arr, origin], {"sp": origin},
        )

    def passed(arr, slot, quarter, send, recv, target):
        view = quarter_at(pairs[arr][1], slot, quarter, width)
        return push(view, view, send.at[arr, slot], recv.at[arr, slot], {"tp": target})

    def start_first(step):
        peer = lax.rem(me + step, sources)
        first(0, peer).start()
        first(1, peer).start()

    loop(1, sources, start_first)
    for copy in owned:
        copy.wait()

    def relay(slot):
        for arr in range(2):
            passed(arr, slot, mine, send_c, recv_c, across).start()
            passed(arr, slot, mine, send_b, recv_b, beside).start()

    relay(me)

    def onward(step):
        slot = lax.rem(me + sources - step, sources)
        for arr in range(2):
            passed(arr, slot, across, send_c, recv_c, across).wait_recv()
            passed(arr, slot, across, send_d, recv_d, beside).start()

    lag = 2

    def steps(step):
        @pl.when(step < sources)
        def _():
            slot = lax.rem(me + sources - step, sources)
            for arr in range(2):
                first_landed(arr, slot).wait_recv()
            relay(slot)

        @pl.when(step >= lag)
        def _():
            onward(step - lag)

    loop(1, sources + lag, steps)

    def finish(slot):
        for arr in range(2):
            passed(arr, slot, beside, send_b, recv_b, beside).wait_recv()
            passed(arr, slot, diagonal, send_d, recv_d, beside).wait_recv()
            passed(arr, slot, mine, send_b, recv_b, beside).wait_send()
            passed(arr, slot, mine, send_c, recv_c, across).wait_send()
            passed(arr, slot, across, send_d, recv_d, beside).wait_send()

    loop(0, sources, finish)

    def finish_first(step):
        peer = lax.rem(me + step, sources)
        for arr in range(2):
            first(arr, peer).wait_send()

    loop(1, sources, finish_first)


def dispatch(sources, slot_inputs, slot_cotan):
    _, capacity, width = slot_inputs.shape
    rows = jax.ShapeDtypeStruct((sources, capacity, 4 * width), slot_inputs.dtype)
    two = pltpu.SemaphoreType.DMA((2, sources))
    return pl.pallas_call(
        functools.partial(dispatch_kernel, sources),
        out_shape=(rows, rows),
        in_specs=[pl.BlockSpec(memory_space=pltpu.VMEM)] * 2,
        out_specs=[pl.BlockSpec(memory_space=pl.ANY)] * 2,
        scratch_shapes=[two] * 8 + [pltpu.SemaphoreType.DMA((2,))],
        compiler_params=pltpu.CompilerParams(collective_id=0, has_side_effects=True),
    )(slot_inputs, slot_cotan)


def return_kernel(
    sources, part_ref, lru_ref, out_ref, olru_ref, near, paired, distant, total,
    send_a, recv_a, send_b, recv_b, send_c, recv_c, send_l, recv_l, local
):
    me, mine = lax.axis_index("sp"), lax.axis_index("tp")
    beside = mine + 1 - 2 * lax.rem(mine, 2)
    across = lax.rem(mine + 2, 4)
    diagonal = lax.rem(beside + 2, 4)
    width = total.shape[2]
    greet(sources, me, (beside, across))

    def load(slot, quarter):
        columns = pl.ds(pl.multiple_of(quarter * width, width), width)
        return part_ref[slot, :, columns].astype(jnp.float32)

    def near_copy(slot, place, quarter):
        return push(
            quarter_at(part_ref, slot, quarter, width), near.at[slot, place],
            send_a.at[slot, place], recv_a.at[slot, place], {"tp": beside},
        )

    def far_copy(slot):
        return push(
            paired.at[slot], distant.at[slot], send_b.at[slot], recv_b.at[slot], {"tp": across}
        )

    def home_copy(peer, slot):
        return push(
            total.at[peer], out_ref.at[slot], send_c.at[peer], recv_c.at[slot], {"sp": peer}
        )

    def own_copy():
        return pltpu.make_async_copy(total.at[me], out_ref.at[me], local.at[0])

    def lru_copy(peer, slot):
        return push(lru_ref, olru_ref.at[slot], send_l.at[peer], recv_l.at[slot], {"sp": peer})

    def start_lru(step):
        peer = lax.rem(me + step, sources)
        lru_copy(peer, me).start()

    lru_own = pltpu.make_async_copy(lru_ref, olru_ref.at[me], local.at[1])
    lru_own.start()
    def begin(step):
        slot = lax.rem(me + 1 + step, sources)
        near_copy(slot, 1, diagonal).start()
        near_copy(slot, 0, beside).start()

    loop(0, sources, begin)
    loop(1, sources, start_lru)
    lag = 2

    def steps(step):
        @pl.when(step < sources)
        def _():
            slot = lax.rem(me + 1 + step, sources)
            near_copy(slot, 1, diagonal).wait_recv()
            paired[slot] = (load(slot, across) + near[slot, 1].astype(jnp.float32)).astype(
                jnp.bfloat16
            )
            far_copy(slot).start()

        @pl.when(step >= lag)
        def _():
            slot = lax.rem(me + 1 + step - lag, sources)
            near_copy(slot, 0, beside).wait_recv()
            far_copy(slot).wait_recv()
            total[slot] = (
                load(slot, mine)
                + near[slot, 0].astype(jnp.float32)
                + distant[slot].astype(jnp.float32)
            ).astype(jnp.bfloat16)

            @pl.when(step < sources + lag - 1)
            def _():
                home_copy(slot, me).start()

    loop(0, sources + lag, steps)
    own_copy().start()

    def finish(step):
        peer = lax.rem(me + step, sources)
        home_copy(peer, peer).wait_recv()
        home_copy(peer, me).wait_send()
        lru_copy(peer, me).wait_send()
        lru_copy(peer, peer).wait_recv()

    loop(1, sources, finish)

    def finish_tp(slot):
        near_copy(slot, 0, beside).wait_send()
        near_copy(slot, 1, diagonal).wait_send()
        far_copy(slot).wait_send()

    loop(0, sources, finish_tp)
    own_copy().wait()
    lru_own.wait()


def return_rows(sources, partial, lru_out):
    _, capacity, model_width = partial.shape
    width = model_width // 4
    held = pltpu.VMEM((sources, capacity, width), jnp.bfloat16)
    two = pltpu.SemaphoreType.DMA((sources, 2))
    one = pltpu.SemaphoreType.DMA((sources,))
    return pl.pallas_call(
        functools.partial(return_kernel, sources),
        out_shape=(
            jax.ShapeDtypeStruct((sources, capacity, width), jnp.bfloat16),
            jax.ShapeDtypeStruct((sources,) + lru_out.shape, lru_out.dtype),
        ),
        in_specs=[pl.BlockSpec(memory_space=pltpu.VMEM)] * 2,
        out_specs=[pl.BlockSpec(memory_space=pl.ANY)] * 2,
        scratch_shapes=[
            pltpu.VMEM((sources, 2, capacity, width), jnp.bfloat16), held, held, held,
            two, two, one, one, one, one, one, one, pltpu.SemaphoreType.DMA((2,)),
        ],
        compiler_params=pltpu.CompilerParams(collective_id=1, has_side_effects=True),
    )(partial, lru_out)


def partner(me, step, sources):
    total = jnp.int32(0)
    for place in range((sources - 1).bit_length()):
        weight = 1 << place
        left = lax.rem(lax.div(me, weight), 2)
        right = lax.rem(lax.div(step, weight), 2) if not isinstance(step, int) else step // weight % 2
        total = total + weight * (left + right - 2 * left * right)
    return total


def announce(sources, me, others):
    barrier = pltpu.get_barrier_semaphore()

    def one(step):
        pl.semaphore_signal(
            barrier, inc=1, device_id={"sp": lax.rem(me + step, sources)}, device_id_type=MESH
        )

    loop(1, sources, one)
    for other in others:
        pl.semaphore_signal(barrier, inc=1, device_id={"tp": other}, device_id_type=MESH)


def all_here(sources, others):
    pl.semaphore_wait(pltpu.get_barrier_semaphore(), sources - 1 + len(others))


def softplus(values):
    return jnp.maximum(values, 0.0) + jnp.log1p(jnp.exp(-jnp.abs(values)))


def minus_expm1(values):
    small = values * (1.0 / 5040.0)
    for divisor in (720.0, 120.0, 24.0, 6.0, 2.0, 1.0):
        small = (small + 1.0 / divisor) * values
    return jnp.where(values > -0.25, -small, 1.0 - jnp.exp(values))


def split_dot(values, maps):
    high = values.astype(jnp.bfloat16)
    rest = values - high.astype(jnp.float32)
    middle = rest.astype(jnp.bfloat16)
    low = (rest - middle.astype(jnp.float32)).astype(jnp.bfloat16)
    return contract(high, maps, 1, 1) + contract(middle, maps, 1, 1) + contract(low, maps, 1, 1)


def scan_rows(coeffs, values, reverse):
    rows = coeffs.shape[0]
    place = lax.broadcasted_iota(jnp.int32, coeffs.shape, 0)
    step = 1
    while step < rows:
        shift = rows - step if reverse else step
        inside = (place < rows - step) if reverse else (place >= step)
        moved_values = jnp.where(inside, pltpu.roll(values, shift, 0), 0.0)
        moved_coeffs = jnp.where(inside, pltpu.roll(coeffs, shift, 0), 1.0)
        values = values + coeffs * moved_values
        coeffs = coeffs * moved_coeffs
        step *= 2
    return coeffs, values


def tail_kernel(
    sources, back, chosen, out_grad, stream, gain, out_proj, lru, conv, branch, dmap, imap,
    dparam, dshift, states, conv_grad, branch_grad, proj_grad,
    normed_grad, grad_b, rows, sums, scale, gates, state_grad, reach, inner,
    send_x, recv_x, send_b, recv_b, send_d, recv_d,
    send_p, recv_p, send_px, recv_px, send_pb, recv_pb, send_pd, recv_pd, send_s, recv_s
):
    me, mine = lax.axis_index("sp"), lax.axis_index("tp")
    beside = mine + 1 - 2 * lax.rem(mine, 2)
    across = lax.rem(mine + 2, 4)
    diagonal = lax.rem(beside + 2, 4)
    tokens, width = out_grad.shape
    quarter = width // 4
    chunk = tokens // 4
    piece = width // sources
    channels = conv.shape[1]
    announce(sources, me, (beside, across))
    normed_grad[mine] = contract(chosen[...], back[...], 1, 0).astype(jnp.bfloat16)
    all_here(sources, (beside, across))

    def part(which, index, send, recv, target):
        view = normed_grad.at[which, pl.ds(index * chunk, chunk)]
        return push(view, view, send.at[index], recv.at[index], {"tp": target})

    for index in range(4):
        part(mine, index, send_x, recv_x, across).start()
        part(mine, index, send_b, recv_b, beside).start()

    def squares(index):
        low = pl.multiple_of(index * 16, 16)
        total = jnp.zeros((16, 1), jnp.float32)
        for q in range(4):
            values = stream[pl.ds(low, 16), q * quarter : (q + 1) * quarter].astype(jnp.float32)
            total = total + jnp.sum(values * values, axis=1, keepdims=True)
        scale[pl.ds(low, 16)] = lax.rsqrt(total / width + norm_eps)

    loop(0, tokens // 16, squares)

    def relay_part(index):
        part(across, index, send_x, recv_x, across).wait_recv()
        part(across, index, send_d, recv_d, beside).start()

    block = 64
    for direction in range(2):
        relay_part(2 * direction)
        base = softplus(-dparam[direction : direction + 1])
        def gate_rows(index):
            low = pl.multiple_of(index * block, block)
            view = pl.ds(low, block)
            held = conv[view]
            decay_gate = jax.nn.sigmoid(contract(held, dmap[direction], 1, 0))
            input_gate = jax.nn.sigmoid(contract(held, imap[direction], 1, 0))
            log_decay = -rate_scale * decay_gate * base + dshift[direction, view]
            gates[4 * direction, view] = decay_gate
            gates[4 * direction + 1, view] = input_gate
            gates[4 * direction + 2, view] = jnp.exp(log_decay)
            gates[4 * direction + 3, view] = jnp.sqrt(minus_expm1(2.0 * log_decay))
        loop(0, tokens // block, gate_rows)
        relay_part(2 * direction + 1)

    def piece_copy(step):
        peer = partner(me, step, sources)
        return push(
            grad_b.at[pl.ds(pl.multiple_of(mine * chunk, chunk), chunk), pl.ds(pl.multiple_of(peer * piece, piece), piece)],
            rows.at[me, pl.ds(pl.multiple_of(mine * chunk, chunk), chunk)],
            send_p.at[step], recv_p.at[step], {"sp": peer},
        )

    def piece_landed(step):
        peer = partner(me, step, sources)
        return push(
            grad_b.at[pl.ds(pl.multiple_of(mine * chunk, chunk), chunk), pl.ds(pl.multiple_of(me * piece, piece), piece)],
            rows.at[peer, pl.ds(pl.multiple_of(mine * chunk, chunk), chunk)],
            send_p.at[step], recv_p.at[step], {"sp": peer},
        )

    def piece_pass(step, which, send, recv, target):
        view = rows.at[partner(me, step, sources), pl.ds(pl.multiple_of(which * chunk, chunk), chunk)]
        return push(view, view, send.at[step], recv.at[step], {"tp": target})

    for index in range(4):
        part(beside, index, send_b, recv_b, beside).wait_recv()
        part(diagonal, index, send_d, recv_d, beside).wait_recv()

        def grad_rows(inside):
            low = pl.multiple_of(index * chunk + inside * 16, 16)
            view = pl.ds(low, 16)
            own_scale = scale[view]
            total = jnp.zeros((16, 1), jnp.float32)
            for q in range(4):
                run = slice(q * quarter, (q + 1) * quarter)
                scaled = gain[:, run].astype(jnp.float32) * normed_grad[q, view].astype(jnp.float32)
                total = total + jnp.sum(
                    stream[view, run].astype(jnp.float32) * scaled, axis=1, keepdims=True
                )
            factor = own_scale * own_scale * total / width
            for q in range(4):
                run = slice(q * quarter, (q + 1) * quarter)
                scaled = gain[:, run].astype(jnp.float32) * normed_grad[q, view].astype(jnp.float32)
                grad_b[view, run] = (
                    out_grad[view, run].astype(jnp.float32)
                    + own_scale * (scaled - stream[view, run].astype(jnp.float32) * factor)
                ).astype(jnp.bfloat16)

        loop(0, chunk // 16, grad_rows)

        @pl.when(mine == index)
        def _():
            loop(1, sources, lambda step: piece_copy(sources - step).start())

    lru_out_grad = contract(grad_b[...], out_proj[...], 1, 0)
    gate = branch[...].astype(jnp.float32)
    slope = 0.7978845608028654
    inside = jnp.tanh(slope * (gate + 0.044715 * gate * gate * gate))
    gelu_gate = 0.5 * gate * (1.0 + inside)
    gelu_slope = 0.5 * (1.0 + inside) + 0.5 * gate * (1.0 - inside * inside) * slope * (
        1.0 + 3.0 * 0.044715 * gate * gate
    )
    branch_grad[...] = lru_out_grad * (states[0] + states[1]) * gelu_slope
    state_grad[...] = lru_out_grad * gelu_gate

    def relay(step):
        piece_landed(step).wait_recv()
        piece_pass(step, mine, send_px, recv_px, across).start()
        piece_pass(step, mine, send_pb, recv_pb, beside).start()

    def onward(step):
        piece_pass(step, across, send_px, recv_px, across).wait_recv()
        piece_pass(step, across, send_pd, recv_pd, beside).start()

    place = lax.broadcasted_iota(jnp.int32, (tokens, channels), 0)
    for direction in range(2):
        decay = gates[4 * direction + 2]
        if direction == 0:
            coeffs = jnp.where(place < tokens - 1, pltpu.roll(decay, tokens - 1, 0), 1.0)
            edge = 0
        else:
            coeffs = jnp.where(place >= 1, pltpu.roll(decay, 1, 0), 1.0)
            edge = tokens - 1
        coeffs, values = scan_rows(coeffs, state_grad[...], direction == 0)
        reach[direction] = coeffs
        inner[direction] = values
        edge_decay = decay[edge : edge + 1]
        sums[me, 2 * direction : 2 * direction + 1] = edge_decay * coeffs[edge : edge + 1]
        sums[me, 2 * direction + 1 : 2 * direction + 2] = edge_decay * values[edge : edge + 1]

    def sums_copy(step, slot):
        return push(
            sums.at[slot], sums.at[slot], send_s.at[step], recv_s.at[step],
            {"sp": partner(me, step, sources)},
        )

    loop(1, sources, lambda step: sums_copy(sources - step, me).start())
    half = sources // 2
    loop(1, half, relay)
    loop(1, half, onward)
    loop(1, sources, lambda step: sums_copy(step, partner(me, step, sources)).wait_recv())
    zero_row = jnp.zeros((1, channels), jnp.float32)

    def from_right(index, carry):
        slot = sources - 1 - index
        ours = sums[slot, 0:1] * carry + sums[slot, 1:2]
        return jnp.where(slot > me, ours, carry)

    def from_left(slot, carry):
        ours = sums[slot, 2:3] * carry + sums[slot, 3:4]
        return jnp.where(slot < me, ours, carry)

    incoming = (
        lax.fori_loop(0, sources, from_right, zero_row),
        lax.fori_loop(0, sources, from_left, zero_row),
    )
    for direction in range(2):
        if direction == 0:
            loop(half, half + half // 2, relay)
        else:
            loop(half + half // 2, sources, relay)
        base = softplus(-dparam[direction : direction + 1])

        def back_rows(index):
            view = pl.ds(pl.multiple_of(index * block, block), block)
            decay_gate, input_gate = gates[4 * direction, view], gates[4 * direction + 1, view]
            decay_rate, drive_scale = gates[4 * direction + 2, view], gates[4 * direction + 3, view]
            conv_float = conv[view].astype(jnp.float32)
            adjoint = inner[direction, view] + reach[direction, view] * incoming[direction]
            driven = input_gate * conv_float
            log_grad = adjoint * (
                states[direction, view] - drive_scale * driven
                - driven * decay_rate * decay_rate / drive_scale
            )
            decay_pre_grad = log_grad * (-rate_scale * base) * decay_gate * (1.0 - decay_gate)
            input_pre_grad = adjoint * drive_scale * driven * (1.0 - input_gate)
            ours = (
                adjoint * drive_scale * input_gate
                + split_dot(decay_pre_grad, dmap[direction])
                + split_dot(input_pre_grad, imap[direction])
            )
            conv_grad[view] = ours if direction == 0 else conv_grad[view] + ours

        loop(0, tokens // block, back_rows)
    loop(half, sources, onward)
    proj_grad[...] = contract(
        grad_b[:, pl.ds(pl.multiple_of(me * piece, piece), piece)], lru[me], 0, 0
    )

    def gather_product(step):
        slot = partner(me, step, sources)
        piece_pass(step, beside, send_pb, recv_pb, beside).wait_recv()
        piece_pass(step, diagonal, send_pd, recv_pd, beside).wait_recv()
        proj_grad[...] += contract(rows[slot], lru[slot], 0, 0)

    loop(1, sources, gather_product)

    def finish(step):
        piece_copy(step).wait_send()
        piece_pass(step, mine, send_px, recv_px, across).wait_send()
        piece_pass(step, mine, send_pb, recv_pb, beside).wait_send()
        piece_pass(step, across, send_pd, recv_pd, beside).wait_send()
        sums_copy(step, me).wait_send()

    loop(1, sources, finish)
    for index in range(4):
        part(mine, index, send_x, recv_x, across).wait_send()
        part(mine, index, send_b, recv_b, beside).wait_send()
        part(across, index, send_d, recv_d, beside).wait_send()


def tail(sources, *operands):
    out_grad, conv = operands[2], operands[7]
    tokens, width = out_grad.shape
    channels = conv.shape[1]
    plane = (tokens, channels)
    four = pltpu.SemaphoreType.DMA((4,))
    each = pltpu.SemaphoreType.DMA((sources,))
    return pl.pallas_call(
        functools.partial(tail_kernel, sources),
        out_shape=(
            jax.ShapeDtypeStruct(plane, jnp.float32),
            jax.ShapeDtypeStruct(plane, jnp.float32),
            jax.ShapeDtypeStruct((width // sources, channels), jnp.float32),
        ),
        in_specs=[pl.BlockSpec(memory_space=pltpu.VMEM)] * len(operands),
        out_specs=[pl.BlockSpec(memory_space=pltpu.VMEM)] * 3,
        scratch_shapes=[
            pltpu.VMEM((4, tokens, width // 4), jnp.bfloat16),
            pltpu.VMEM((tokens, width), jnp.bfloat16),
            pltpu.VMEM((sources, tokens, width // sources), jnp.bfloat16),
            pltpu.VMEM((sources, 8, channels), jnp.float32),
            pltpu.VMEM((tokens, 1), jnp.float32),
            pltpu.VMEM((8,) + plane, jnp.float32),
            pltpu.VMEM(plane, jnp.float32),
            pltpu.VMEM((2,) + plane, jnp.float32),
            pltpu.VMEM((2,) + plane, jnp.float32),
        ] + [four] * 6 + [each] * 10,
        compiler_params=pltpu.CompilerParams(collective_id=2, has_side_effects=True),
    )(*operands)


def body(
    out_grad,
    stream,
    norm_gain,
    routes,
    route_weight,
    gate_weight,
    up_weight,
    down_weight,
    out_proj,
    conv_out,
    gate_branch,
    decay_map,
    input_map,
    decay_param,
    decay_shift,
    states,
):
    sources = lax.axis_size("sp")
    quarters = lax.axis_size("tp")
    experts = EXP_DEV * sources
    capacity = (5 * TOP * TOK_DEV + 4 * experts - 1) // (4 * experts)
    token_count, model_width = stream.shape
    stream_f = stream.astype(jnp.float32)
    row_scale = lax.rsqrt(jnp.mean(stream_f * stream_f, axis=1, keepdims=True) + norm_eps)
    unit_rows = stream_f * row_scale
    gain_row = norm_gain.astype(jnp.float32)[None, :]
    normed = (unit_rows * gain_row).astype(jnp.bfloat16)
    pair_expert = routes.reshape(-1)
    pair_count = pair_expert.shape[0]
    onehot = (pair_expert[:, None] == jnp.arange(experts, dtype=jnp.int32)[None, :]).astype(
        jnp.int32
    )
    slot_rank = jnp.sum((jnp.cumsum(onehot, axis=0) - onehot) * onehot, axis=1)
    slot_index = pair_expert * capacity + slot_rank
    places = slot_index.reshape(token_count, TOP, 1) == jnp.arange(
        experts * capacity, dtype=jnp.int32
    )
    chosen = jnp.any(places, axis=1).astype(jnp.bfloat16)
    slot_weight = jnp.sum(jnp.where(places, route_weight[:, :, None], 0.0), axis=(0, 1))[:, None]
    column_width = model_width // quarters
    column_start = lax.axis_index("tp") * column_width
    normed_cols = lax.dynamic_slice_in_dim(normed, column_start, column_width, 1)
    grad_cols = lax.dynamic_slice_in_dim(out_grad, column_start, column_width, 1)
    slot_inputs = contract(chosen, normed_cols, 0, 0).astype(jnp.bfloat16)
    slot_cotan = (slot_weight * contract(chosen, grad_cols, 0, 0)).astype(jnp.bfloat16)
    total_state = states[0] + states[1]
    gate_float = gate_branch.astype(jnp.float32)
    gelu_gate = jax.nn.gelu(gate_float)
    lru_out = (total_state * gelu_gate).astype(jnp.bfloat16)
    got_inputs, got_cotan = dispatch(
        sources,
        slot_inputs.reshape(sources, capacity, column_width),
        slot_cotan.reshape(sources, capacity, column_width),
    )
    expert_inputs = got_inputs.reshape(1, sources * capacity, model_width)
    expert_cotan = got_cotan.reshape(1, sources * capacity, model_width)
    gate_grads, up_grads, down_grads, partials = ([], [], [], [])
    gate_wgrad, up_wgrad, down_wgrad, gate_grad, up_grad = expert_pass(
        expert_inputs[0], expert_cotan[0], gate_weight[0], up_weight[0], down_weight[0]
    )
    gate_grads.append(gate_wgrad.astype(jnp.bfloat16))
    up_grads.append(up_wgrad.astype(jnp.bfloat16))
    down_grads.append(down_wgrad.astype(jnp.bfloat16))
    partials.append(
        (contract(gate_grad, gate_weight[0], 1, 1) + contract(up_grad, up_weight[0], 1, 1)).astype(
            jnp.bfloat16
        )
    )
    part_back, lru_rows = return_rows(
        sources, partials[0].reshape(sources, capacity, model_width), lru_out
    )
    conv_grad, gate_branch_grad, out_proj_grad = tail(
        sources,
        part_back.reshape(sources * capacity, column_width),
        chosen,
        out_grad,
        stream,
        norm_gain[None, :],
        out_proj,
        lru_rows,
        conv_out,
        gate_branch,
        decay_map[:, 0],
        input_map[:, 0],
        decay_param,
        decay_shift,
        states,
    )
    return (
        conv_grad,
        gate_branch_grad,
        out_proj_grad,
        jnp.stack(gate_grads),
        jnp.stack(up_grads),
        jnp.stack(down_grads),
    )


def solution(mesh):
    placed = (
        P("sp", None),
        P("sp", None),
        P(),
        P("sp", None),
        P("sp", None),
        P("sp", None, "tp"),
        P("sp", None, "tp"),
        P("sp", "tp", None),
        P(None, "tp"),
        P("sp", "tp"),
        P("sp", "tp"),
        P(None, "tp", None, None),
        P(None, "tp", None, None),
        P(None, "tp"),
        P(None, "sp", "tp"),
        P(None, "sp", "tp"),
    )
    return jax.shard_map(
        body,
        mesh=mesh,
        in_specs=placed,
        out_specs=(
            P("sp", "tp"),
            P("sp", "tp"),
            P("sp", "tp"),
            P("sp", None, "tp"),
            P("sp", None, "tp"),
            P("sp", "tp", None),
        ),
        check_vma=False,
    )
```

```python
import functools

import jax
import jax.numpy as jnp
from jax import lax
from jax.experimental import pallas as pl
from jax.experimental.pallas import tpu as pltpu
from jax.sharding import PartitionSpec as P

TOP = 2
EXP_DEV = 1
TOK_DEV = 256


rate_scale = 8.0
norm_eps = 1e-06


def contract(left, right, left_dim, right_dim):
    return lax.dot_general(
        left, right, (((left_dim,), (right_dim,)), ((), ())), preferred_element_type=jnp.float32
    )


MESH = pl.DeviceIdType.MESH


def push(source, target, send_sem, recv_sem, where):
    return pltpu.make_async_remote_copy(
        src_ref=source,
        dst_ref=target,
        send_sem=send_sem,
        recv_sem=recv_sem,
        device_id=where,
        device_id_type=MESH,
    )


def loop(low, high, step):
    def one(index, carry):
        step(index)
        return carry

    lax.fori_loop(low, high, one, 0)


def partner(me, step, sources):
    total = jnp.int32(0)
    for place in range((sources - 1).bit_length()):
        weight = 1 << place
        left = lax.rem(lax.div(me, weight), 2)
        right = lax.rem(lax.div(step, weight), 2) if not isinstance(step, int) else step // weight % 2
        total = total + weight * (left + right - 2 * left * right)
    return total


def announce(sources, me, others):
    barrier = pltpu.get_barrier_semaphore()

    def one(step):
        pl.semaphore_signal(
            barrier, inc=1, device_id={"sp": lax.rem(me + step, sources)}, device_id_type=MESH
        )

    loop(1, sources, one)
    for other in others:
        pl.semaphore_signal(barrier, inc=1, device_id={"tp": other}, device_id_type=MESH)


def all_here(sources, others):
    pl.semaphore_wait(pltpu.get_barrier_semaphore(), sources - 1 + len(others))


def softplus(values):
    return jnp.maximum(values, 0.0) + jnp.log1p(jnp.exp(-jnp.abs(values)))


def minus_expm1(values):
    small = values * (1.0 / 5040.0)
    for divisor in (720.0, 120.0, 24.0, 6.0, 2.0, 1.0):
        small = (small + 1.0 / divisor) * values
    return jnp.where(values > -0.25, -small, 1.0 - jnp.exp(values))


def split_dot(values, maps):
    high = values.astype(jnp.bfloat16)
    rest = values - high.astype(jnp.float32)
    middle = rest.astype(jnp.bfloat16)
    low = (rest - middle.astype(jnp.float32)).astype(jnp.bfloat16)
    return contract(high, maps, 1, 1) + contract(middle, maps, 1, 1) + contract(low, maps, 1, 1)


def scan_rows(coeffs, values, reverse):
    rows = coeffs.shape[0]
    place = lax.broadcasted_iota(jnp.int32, coeffs.shape, 0)
    step = 1
    while step < rows:
        shift = rows - step if reverse else step
        inside = (place < rows - step) if reverse else (place >= step)
        moved_values = jnp.where(inside, pltpu.roll(values, shift, 0), 0.0)
        moved_coeffs = jnp.where(inside, pltpu.roll(coeffs, shift, 0), 1.0)
        values = values + coeffs * moved_values
        coeffs = coeffs * moved_coeffs
        step *= 2
    return coeffs, values


def front_kernel(
    sources, capacity, stream, out_grad, gain, routes, weights, gate_hbm, up_hbm, down_hbm,
    row_grad, gate_out, up_out, down_out,
    gate_w, up_w, down_w, gate_wg, up_wg, down_wg,
    place, slot_weight, normed, send_in, send_ct, rows_in, rows_ct, part, near, distant, back,
    hidden, pre_grad,
    load, store, send_a, recv_a, send_b, recv_b, send_c, recv_c, send_d, recv_d,
    send_n, recv_n, send_f, recv_f, send_h, recv_h
):
    me, mine = lax.axis_index("sp"), lax.axis_index("tp")
    beside = mine + 1 - 2 * lax.rem(mine, 2)
    across = lax.rem(mine + 2, 4)
    diagonal = lax.rem(beside + 2, 4)
    tokens, model = stream.shape
    width = model // 4
    units = gate_w.shape[1]
    slots = sources * capacity
    announce(sources, me, (beside, across))
    loads = [
        pltpu.make_async_copy(src, dst, load.at[index])
        for index, (src, dst) in enumerate(((gate_hbm, gate_w), (up_hbm, up_w), (down_hbm, down_w)))
    ]
    for copy in loads:
        copy.start()

    def columns(which):
        return pl.ds(pl.multiple_of(which * width, width), width)

    def rows_of(slot):
        return pl.ds(pl.multiple_of(slot * capacity, capacity), capacity)

    expert = lax.broadcasted_iota(jnp.int32, (128, tokens), 0)
    chosen = jnp.where((routes[0:1] == expert) | (routes[1:2] == expert), 1.0, 0.0).astype(
        jnp.bfloat16
    )
    earlier = lax.broadcasted_iota(jnp.int32, (tokens, tokens), 0) < lax.broadcasted_iota(
        jnp.int32, (tokens, tokens), 1
    )
    rank = contract(chosen, jnp.where(earlier, 1.0, 0.0).astype(jnp.bfloat16), 1, 0).astype(
        jnp.bfloat16
    )
    slot_row = lax.broadcasted_iota(jnp.int32, (slots, 128), 0)
    slot_lane = lax.broadcasted_iota(jnp.int32, (slots, 128), 1)
    slot_low = slot_lane * capacity
    owner = (slot_row >= slot_low) & (slot_row < slot_low + capacity)
    named = jnp.sum(jnp.where(owner, slot_lane.astype(jnp.float32), 0.0), axis=1, keepdims=True)
    offset = jnp.sum(
        jnp.where(owner, (slot_row - slot_low).astype(jnp.float32), 0.0), axis=1, keepdims=True
    )
    ranks = contract(jnp.where(owner, 1.0, 0.0).astype(jnp.bfloat16), rank, 1, 0)
    fits = ranks == offset
    first_is = (routes[0:1].astype(jnp.float32) == named) & fits
    second_is = (routes[1:2].astype(jnp.float32) == named) & fits
    place[...] = jnp.where(first_is | second_is, 1.0, 0.0).astype(jnp.bfloat16)
    slot_weight[...] = jnp.sum(
        jnp.where(first_is, weights[0:1], 0.0) + jnp.where(second_is, weights[1:2], 0.0),
        axis=1, keepdims=True,
    )

    def norm_rows(index):
        view = pl.ds(pl.multiple_of(index * 16, 16), 16)
        total = jnp.zeros((16, 1), jnp.float32)
        for q in range(4):
            values = stream[view, q * width : (q + 1) * width].astype(jnp.float32)
            total = total + jnp.sum(values * values, axis=1, keepdims=True)
        row_scale = lax.rsqrt(total / model + norm_eps)
        for q in range(4):
            run = slice(q * width, (q + 1) * width)
            normed[view, run] = (
                stream[view, run].astype(jnp.float32) * row_scale * gain[:, run].astype(jnp.float32)
            ).astype(jnp.bfloat16)

    all_here(sources, (beside, across))
    pairs = ((send_in, rows_in), (send_ct, rows_ct))

    def first(arr, step, slot, quarter, owner_slot):
        src, dst = pairs[arr]
        return push(
            src.at[slot], dst.at[rows_of(owner_slot), columns(quarter)],
            send_a.at[arr, slot], recv_a.at[arr, slot], {"sp": partner(me, step, sources)},
        )

    def give_ct(step, slot, quarter):
        view = rows_of(partner(me, step, sources))
        send_ct[slot] = (
            slot_weight[view] * contract(place[view], out_grad[:, columns(quarter)], 1, 0)
        ).astype(jnp.bfloat16)
        first(1, step, slot, quarter, me).start()

    def give_in(step, slot, quarter):
        view = rows_of(partner(me, step, sources))
        send_in[slot] = contract(place[view], normed[:, columns(quarter)], 1, 0).astype(
            jnp.bfloat16
        )
        first(0, step, slot, quarter, me).start()

    def give(step):
        give_ct(step, step, mine)
        give_in(step, step, mine)

    half = sources // 2
    place_z = lax.div(me * 4, sources)
    at_end = (place_z == 0) | (place_z == 3)

    def nth(index):
        return 2 + lax.rem(index + jnp.where(at_end, 0, half - 2), sources - 2)

    def give_second(step):
        give_ct(step, sources - 1 + step, across)
        give_in(step, sources - 1 + step, across)

    give_ct(1, 1, mine)
    give_ct(nth(0), nth(0), mine)
    loop(0, tokens // 16, norm_rows)
    give_in(1, 1, mine)
    give_in(nth(0), nth(0), mine)

    loop(1, sources - 2, lambda index: give(nth(index)))
    give_second(1)
    own = rows_of(me)

    def own_columns(quarter):
        picked = place[own]
        rows_in[own, columns(quarter)] = contract(picked, normed[:, columns(quarter)], 1, 0).astype(
            jnp.bfloat16
        )
        rows_ct[own, columns(quarter)] = (
            slot_weight[own] * contract(picked, out_grad[:, columns(quarter)], 1, 0)
        ).astype(jnp.bfloat16)

    loop(0, 4, own_columns)

    def passed(arr, step, quarter, send, recv, target):
        view = pairs[arr][1].at[rows_of(partner(me, step, sources)), columns(quarter)]
        return push(view, view, send.at[arr, step], recv.at[arr, step], {"tp": target})

    def relay(step):
        slot = partner(me, step, sources)
        for arr in range(2):
            first(arr, step, step, mine, slot).wait_recv()
            passed(arr, step, mine, send_c, recv_c, across).start()
            passed(arr, step, mine, send_b, recv_b, beside).start()

    def onward(step):
        for arr in range(2):
            passed(arr, step, across, send_c, recv_c, across).wait_recv()
            passed(arr, step, across, send_d, recv_d, beside).start()

    def complete(step):
        for arr in range(2):
            passed(arr, step, beside, send_b, recv_b, beside).wait_recv()
            passed(arr, step, diagonal, send_d, recv_d, beside).wait_recv()

    def compute(step):
        view = rows_of(partner(me, step, sources))
        inputs = rows_in[view]
        gate_pre = contract(inputs, gate_w[...], 1, 0)
        up_pre = contract(inputs, up_w[...], 1, 0)
        logistic = jax.nn.sigmoid(gate_pre)
        gated = gate_pre * logistic
        hidden[view] = (gated * up_pre).astype(jnp.bfloat16)
        hidden_grad = contract(rows_ct[view], down_w[...], 1, 1)
        up_grad = (hidden_grad * gated).astype(jnp.bfloat16)
        gate_grad = (
            hidden_grad * up_pre * (logistic * (1.0 + gate_pre * (1.0 - logistic)))
        ).astype(jnp.bfloat16)
        pre_grad[view, :units] = gate_grad
        pre_grad[view, units:] = up_grad

        def back_columns(quarter):
            rows = columns(quarter)
            part[view, rows] = (
                contract(gate_grad, gate_w[rows], 1, 1) + contract(up_grad, up_w[rows], 1, 1)
            ).astype(jnp.bfloat16)

        loop(0, 4, back_columns)

    def part_of(step, quarter):
        return part[rows_of(partner(me, step, sources)), columns(quarter)].astype(jnp.float32)

    def near_copy(step, half, quarter):
        return push(
            part.at[rows_of(partner(me, step, sources)), columns(quarter)], near.at[step, half],
            send_n.at[step, half], recv_n.at[step, half], {"tp": beside},
        )

    def far_copy(step):
        return push(
            send_in.at[step], distant.at[step], send_f.at[step], recv_f.at[step], {"tp": across}
        )

    def home_copy(step, slot):
        return push(
            send_ct.at[step], back.at[rows_of(slot)], send_h.at[step], recv_h.at[step],
            {"sp": partner(me, step, sources)},
        )

    def share_near(step):
        near_copy(step, 1, diagonal).start()
        near_copy(step, 0, beside).start()

    def share_far(step):
        near_copy(step, 1, diagonal).wait_recv()

        @pl.when(step > 0)
        def _():
            first(0, step, step, mine, me).wait_send()

        send_in[step] = (part_of(step, across) + near[step, 1].astype(jnp.float32)).astype(
            jnp.bfloat16
        )
        far_copy(step).start()

    def send_home(step):
        near_copy(step, 0, beside).wait_recv()
        far_copy(step).wait_recv()
        total = (
            part_of(step, mine)
            + near[step, 0].astype(jnp.float32)
            + distant[step].astype(jnp.float32)
        ).astype(jnp.bfloat16)

        @pl.when(step > 0)
        def _():
            first(1, step, step, mine, me).wait_send()
            send_ct[step] = total
            home_copy(step, me).start()

        @pl.when(step == 0)
        def _():
            back[own] = total

    for copy in loads:
        copy.wait()

    def turn(index):
        far = jnp.where(at_end, index + sources - 3, index + half - 1)
        late = jnp.where(at_end | (index < half + 2), index - 2, index)
        step = jnp.where(index < 3, index + 1, jnp.where(index == 3, 1, jnp.where(index < 6, far - 3, late)))
        return jnp.where(index == 0, 0, step)

    def relay_turn(index):
        step = turn(index)

        @pl.when(step == 1)
        def _():
            slot = partner(me, step, sources)
            for arr in range(2):
                first(arr, step, step, mine, slot).wait_recv()
                passed(arr, step, mine, send_b, recv_b, beside).start()
            for arr in range(2):
                first(arr, step, sources - 1 + step, across, slot).wait_recv()
                passed(arr, step, across, send_d, recv_d, beside).start()

        @pl.when(step > 1)
        def _():
            relay(step)

    def onward_turn(index):
        @pl.when(turn(index) > 1)
        def _():
            onward(turn(index))

    def stage(index):
        step = turn(index)

        @pl.when(index > 0)
        def _():
            complete(step)

        compute(step)
        share_near(step)
        share_far(step)

        @pl.when(index == 0)
        def _():
            relay_turn(1)

        @pl.when(index + 2 < sources)
        def _():
            relay_turn(index + 2)

        @pl.when(index + 1 < sources)
        def _():
            onward_turn(index + 1)

        @pl.when(index > 0)
        def _():
            send_home(turn(index - 1))

    loop(0, sources, stage)
    run = model // 8

    def stored(index):
        view = pl.ds(pl.multiple_of(index * run, run), run)
        return [
            pltpu.make_async_copy(src.at[where], dst.at[where], store.at[arr, index])
            for arr, (src, dst, where) in enumerate(
                ((gate_wg, gate_out, view), (up_wg, up_out, view), (down_wg, down_out, (slice(None), view)))
            )
        ]

    def weight_run(index):
        view = pl.ds(pl.multiple_of(index * run, run), run)
        both = contract(rows_in[:, view], pre_grad[...], 0, 0).astype(jnp.bfloat16)
        gate_wg[view] = both[:, :units]
        up_wg[view] = both[:, units:]
        down_wg[:, view] = contract(hidden[...], rows_ct[:, view], 0, 0).astype(jnp.bfloat16)
        for copy in stored(index):
            copy.start()

    loop(0, 5, weight_run)
    send_home(turn(sources - 1))
    loop(5, 8, weight_run)

    def finish_home(step):
        home_copy(step, partner(me, step, sources)).wait_recv()

    loop(1, sources, finish_home)
    row_grad[...] = contract(place[...], back[...], 0, 0).astype(jnp.bfloat16)

    def finish_sends(step):
        near_copy(step, 0, beside).wait_send()
        near_copy(step, 1, diagonal).wait_send()
        far_copy(step).wait_send()

        @pl.when(step > 0)
        def _():
            home_copy(step, me).wait_send()
            for arr in range(2):
                passed(arr, step, mine, send_b, recv_b, beside).wait_send()
                passed(arr, step, across, send_d, recv_d, beside).wait_send()

        @pl.when(step > 1)
        def _():
            for arr in range(2):
                passed(arr, step, mine, send_c, recv_c, across).wait_send()

    loop(0, sources, finish_sends)
    for step in range(1, 2):
        for arr in range(2):
            first(arr, step, sources - 1 + step, across, me).wait_send()

    def finish_stores(index):
        for copy in stored(index):
            copy.wait()

    loop(0, 8, finish_stores)


def front(sources, capacity, *operands):
    stream, gate_weight, down_weight = operands[0], operands[5], operands[7]
    tokens, model = stream.shape
    units = gate_weight.shape[1]
    slots, width = sources * capacity, model // 4
    narrow = jnp.bfloat16
    vmem, anywhere = pl.BlockSpec(memory_space=pltpu.VMEM), pl.BlockSpec(memory_space=pl.ANY)
    tall, wide = gate_weight.shape, down_weight.shape
    dma = pltpu.SemaphoreType.DMA
    return pl.pallas_call(
        functools.partial(front_kernel, sources, capacity),
        out_shape=(
            jax.ShapeDtypeStruct((tokens, width), narrow),
            jax.ShapeDtypeStruct(tall, narrow),
            jax.ShapeDtypeStruct(tall, narrow),
            jax.ShapeDtypeStruct(wide, narrow),
        ),
        in_specs=[vmem] * 5 + [anywhere] * 3,
        out_specs=[vmem] + [anywhere] * 3,
        scratch_shapes=[
            pltpu.VMEM(tall, narrow), pltpu.VMEM(tall, narrow), pltpu.VMEM(wide, narrow),
            pltpu.VMEM(tall, narrow), pltpu.VMEM(tall, narrow), pltpu.VMEM(wide, narrow),
            pltpu.VMEM((slots, tokens), narrow),
            pltpu.VMEM((slots, 1), jnp.float32),
            pltpu.VMEM((tokens, model), narrow),
            pltpu.VMEM((sources + 1, capacity, width), narrow),
            pltpu.VMEM((sources + 1, capacity, width), narrow),
            pltpu.VMEM((slots, model), narrow),
            pltpu.VMEM((slots, model), narrow),
            pltpu.VMEM((slots, model), narrow),
            pltpu.VMEM((sources, 2, capacity, width), narrow),
            pltpu.VMEM((sources, capacity, width), narrow),
            pltpu.VMEM((slots, width), narrow),
            pltpu.VMEM((slots, units), narrow),
            pltpu.VMEM((slots, 2 * units), narrow),
            dma((3,)), dma((3, 8)), dma((2, sources + 1)), dma((2, sources + 1)),
        ] + [dma((2, sources))] * 6 + [dma((sources, 2))] * 2 + [dma((sources,))] * 4,
        compiler_params=pltpu.CompilerParams(
            collective_id=0, has_side_effects=True, vmem_limit_bytes=67043328
        ),
    )(*operands)


def settle_kernel(*refs):
    count = (len(refs) - 2) // 3
    load, store = refs[-2:]
    loads = [pltpu.make_async_copy(refs[i], refs[2 * count + i], load.at[i]) for i in range(count)]
    stores = [
        pltpu.make_async_copy(refs[2 * count + i], refs[count + i], store.at[i])
        for i in range(count)
    ]
    for copy in loads:
        copy.start()
    for before, after in zip(loads, stores):
        before.wait()
        after.start()
    for copy in stores:
        copy.wait()


def settle(*arrays):
    anywhere = pl.BlockSpec(memory_space=pl.ANY)
    dma = pltpu.SemaphoreType.DMA((len(arrays),))
    return pl.pallas_call(
        settle_kernel,
        out_shape=tuple(jax.ShapeDtypeStruct(a.shape, a.dtype) for a in arrays),
        in_specs=[anywhere] * len(arrays),
        out_specs=[anywhere] * len(arrays),
        scratch_shapes=[pltpu.VMEM(a.shape, a.dtype) for a in arrays] + [dma, dma],
    )(*arrays)


def tail_kernel(
    sources, row_grad, out_grad, stream, gain, out_proj, conv, branch, dmap, imap,
    dparam, dshift, states, conv_grad, branch_grad, proj_grad,
    normed_grad, grad_b, rows, sums, lru, scale, gates, state_grad, reach, inner,
    send_x, recv_x, send_b, recv_b, send_d, recv_d,
    send_p, recv_p, send_px, recv_px, send_pb, recv_pb, send_pd, recv_pd, send_s, recv_s,
    send_l, recv_l
):
    me, mine = lax.axis_index("sp"), lax.axis_index("tp")
    beside = mine + 1 - 2 * lax.rem(mine, 2)
    across = lax.rem(mine + 2, 4)
    diagonal = lax.rem(beside + 2, 4)
    tokens, width = out_grad.shape
    quarter = width // 4
    chunk = tokens // 4
    piece = width // sources
    channels = conv.shape[1]
    announce(sources, me, (beside, across))
    normed_grad[mine] = row_grad[...]
    gate = branch[...].astype(jnp.float32)
    slope = 0.7978845608028654
    inside = jnp.tanh(slope * (gate + 0.044715 * gate * gate * gate))
    lru[me] = ((states[0] + states[1]) * (0.5 * gate * (1.0 + inside))).astype(jnp.bfloat16)
    all_here(sources, (beside, across))

    def part(which, index, send, recv, target):
        view = normed_grad.at[which, pl.ds(index * chunk, chunk)]
        return push(view, view, send.at[index], recv.at[index], {"tp": target})

    for index in range(4):
        part(mine, index, send_x, recv_x, across).start()
        part(mine, index, send_b, recv_b, beside).start()

    def lru_copy(step, slot):
        return push(
            lru.at[slot], lru.at[slot], send_l.at[step], recv_l.at[step],
            {"sp": partner(me, step, sources)},
        )

    loop(1, sources, lambda step: lru_copy(step, me).start())

    def squares(index):
        low = pl.multiple_of(index * 16, 16)
        total = jnp.zeros((16, 1), jnp.float32)
        for q in range(4):
            values = stream[pl.ds(low, 16), q * quarter : (q + 1) * quarter].astype(jnp.float32)
            total = total + jnp.sum(values * values, axis=1, keepdims=True)
        scale[pl.ds(low, 16)] = lax.rsqrt(total / width + norm_eps)

    loop(0, tokens // 16, squares)

    def relay_part(index):
        part(across, index, send_x, recv_x, across).wait_recv()
        part(across, index, send_d, recv_d, beside).start()

    block = 64
    for direction in range(2):
        relay_part(2 * direction)
        base = softplus(-dparam[direction : direction + 1])
        def gate_rows(index):
            low = pl.multiple_of(index * block, block)
            view = pl.ds(low, block)
            held = conv[view]
            decay_gate = jax.nn.sigmoid(contract(held, dmap[direction], 1, 0))
            input_gate = jax.nn.sigmoid(contract(held, imap[direction], 1, 0))
            log_decay = -rate_scale * decay_gate * base + dshift[direction, view]
            gates[4 * direction, view] = decay_gate
            gates[4 * direction + 1, view] = input_gate
            gates[4 * direction + 2, view] = jnp.exp(log_decay)
            gates[4 * direction + 3, view] = jnp.sqrt(minus_expm1(2.0 * log_decay))
        loop(0, tokens // block, gate_rows)
        relay_part(2 * direction + 1)

    def piece_copy(step):
        peer = partner(me, step, sources)
        return push(
            grad_b.at[pl.ds(pl.multiple_of(mine * chunk, chunk), chunk), pl.ds(pl.multiple_of(peer * piece, piece), piece)],
            rows.at[me, pl.ds(pl.multiple_of(mine * chunk, chunk), chunk)],
            send_p.at[step], recv_p.at[step], {"sp": peer},
        )

    def piece_landed(step):
        peer = partner(me, step, sources)
        return push(
            grad_b.at[pl.ds(pl.multiple_of(mine * chunk, chunk), chunk), pl.ds(pl.multiple_of(me * piece, piece), piece)],
            rows.at[peer, pl.ds(pl.multiple_of(mine * chunk, chunk), chunk)],
            send_p.at[step], recv_p.at[step], {"sp": peer},
        )

    def piece_pass(step, which, send, recv, target):
        view = rows.at[partner(me, step, sources), pl.ds(pl.multiple_of(which * chunk, chunk), chunk)]
        return push(view, view, send.at[step], recv.at[step], {"tp": target})

    for index in range(4):
        part(beside, index, send_b, recv_b, beside).wait_recv()
        part(diagonal, index, send_d, recv_d, beside).wait_recv()

        def grad_rows(inside):
            low = pl.multiple_of(index * chunk + inside * 16, 16)
            view = pl.ds(low, 16)
            own_scale = scale[view]
            total = jnp.zeros((16, 1), jnp.float32)
            for q in range(4):
                run = slice(q * quarter, (q + 1) * quarter)
                scaled = gain[:, run].astype(jnp.float32) * normed_grad[q, view].astype(jnp.float32)
                total = total + jnp.sum(
                    stream[view, run].astype(jnp.float32) * scaled, axis=1, keepdims=True
                )
            factor = own_scale * own_scale * total / width
            for q in range(4):
                run = slice(q * quarter, (q + 1) * quarter)
                scaled = gain[:, run].astype(jnp.float32) * normed_grad[q, view].astype(jnp.float32)
                grad_b[view, run] = (
                    out_grad[view, run].astype(jnp.float32)
                    + own_scale * (scaled - stream[view, run].astype(jnp.float32) * factor)
                ).astype(jnp.bfloat16)

        loop(0, chunk // 16, grad_rows)

        @pl.when(mine == index)
        def _():
            loop(1, sources, lambda step: piece_copy(sources - step).start())

    lru_out_grad = contract(grad_b[...], out_proj[...], 1, 0)
    gate = branch[...].astype(jnp.float32)
    slope = 0.7978845608028654
    inside = jnp.tanh(slope * (gate + 0.044715 * gate * gate * gate))
    gelu_gate = 0.5 * gate * (1.0 + inside)
    gelu_slope = 0.5 * (1.0 + inside) + 0.5 * gate * (1.0 - inside * inside) * slope * (
        1.0 + 3.0 * 0.044715 * gate * gate
    )
    branch_grad[...] = lru_out_grad * (states[0] + states[1]) * gelu_slope
    state_grad[...] = lru_out_grad * gelu_gate

    def relay(step):
        piece_landed(step).wait_recv()
        piece_pass(step, mine, send_px, recv_px, across).start()
        piece_pass(step, mine, send_pb, recv_pb, beside).start()

    def onward(step):
        piece_pass(step, across, send_px, recv_px, across).wait_recv()
        piece_pass(step, across, send_pd, recv_pd, beside).start()

    place = lax.broadcasted_iota(jnp.int32, (tokens, channels), 0)
    for direction in range(2):
        decay = gates[4 * direction + 2]
        if direction == 0:
            coeffs = jnp.where(place < tokens - 1, pltpu.roll(decay, tokens - 1, 0), 1.0)
            edge = 0
        else:
            coeffs = jnp.where(place >= 1, pltpu.roll(decay, 1, 0), 1.0)
            edge = tokens - 1
        coeffs, values = scan_rows(coeffs, state_grad[...], direction == 0)
        reach[direction] = coeffs
        inner[direction] = values
        edge_decay = decay[edge : edge + 1]
        sums[me, 2 * direction : 2 * direction + 1] = edge_decay * coeffs[edge : edge + 1]
        sums[me, 2 * direction + 1 : 2 * direction + 2] = edge_decay * values[edge : edge + 1]

    def sums_copy(step, slot):
        return push(
            sums.at[slot], sums.at[slot], send_s.at[step], recv_s.at[step],
            {"sp": partner(me, step, sources)},
        )

    loop(1, sources, lambda step: sums_copy(sources - step, me).start())
    half = sources // 2
    loop(1, half, relay)
    loop(1, half, onward)
    loop(1, sources, lambda step: sums_copy(step, partner(me, step, sources)).wait_recv())
    zero_row = jnp.zeros((1, channels), jnp.float32)

    def from_right(index, carry):
        slot = sources - 1 - index
        ours = sums[slot, 0:1] * carry + sums[slot, 1:2]
        return jnp.where(slot > me, ours, carry)

    def from_left(slot, carry):
        ours = sums[slot, 2:3] * carry + sums[slot, 3:4]
        return jnp.where(slot < me, ours, carry)

    incoming = (
        lax.fori_loop(0, sources, from_right, zero_row),
        lax.fori_loop(0, sources, from_left, zero_row),
    )
    for direction in range(2):
        if direction == 0:
            loop(half, half + half // 2, relay)
        else:
            loop(half + half // 2, sources, relay)
        base = softplus(-dparam[direction : direction + 1])

        def back_rows(index):
            view = pl.ds(pl.multiple_of(index * block, block), block)
            decay_gate, input_gate = gates[4 * direction, view], gates[4 * direction + 1, view]
            decay_rate, drive_scale = gates[4 * direction + 2, view], gates[4 * direction + 3, view]
            conv_float = conv[view].astype(jnp.float32)
            adjoint = inner[direction, view] + reach[direction, view] * incoming[direction]
            driven = input_gate * conv_float
            log_grad = adjoint * (
                states[direction, view] - drive_scale * driven
                - driven * decay_rate * decay_rate / drive_scale
            )
            decay_pre_grad = log_grad * (-rate_scale * base) * decay_gate * (1.0 - decay_gate)
            input_pre_grad = adjoint * drive_scale * driven * (1.0 - input_gate)
            ours = (
                adjoint * drive_scale * input_gate
                + split_dot(decay_pre_grad, dmap[direction])
                + split_dot(input_pre_grad, imap[direction])
            )
            conv_grad[view] = ours if direction == 0 else conv_grad[view] + ours

        loop(0, tokens // block, back_rows)
    loop(half, sources, onward)
    proj_grad[...] = contract(
        grad_b[:, pl.ds(pl.multiple_of(me * piece, piece), piece)], lru[me], 0, 0
    )

    def gather_product(step):
        slot = partner(me, step, sources)
        lru_copy(step, slot).wait_recv()
        piece_pass(step, beside, send_pb, recv_pb, beside).wait_recv()
        piece_pass(step, diagonal, send_pd, recv_pd, beside).wait_recv()
        proj_grad[...] += contract(rows[slot], lru[slot], 0, 0)

    loop(1, sources, gather_product)

    def finish(step):
        piece_copy(step).wait_send()
        piece_pass(step, mine, send_px, recv_px, across).wait_send()
        piece_pass(step, mine, send_pb, recv_pb, beside).wait_send()
        piece_pass(step, across, send_pd, recv_pd, beside).wait_send()
        sums_copy(step, me).wait_send()
        lru_copy(step, me).wait_send()

    loop(1, sources, finish)
    for index in range(4):
        part(mine, index, send_x, recv_x, across).wait_send()
        part(mine, index, send_b, recv_b, beside).wait_send()
        part(across, index, send_d, recv_d, beside).wait_send()


def tail(sources, *operands):
    out_grad, conv = operands[1], operands[5]
    tokens, width = out_grad.shape
    channels = conv.shape[1]
    plane = (tokens, channels)
    four = pltpu.SemaphoreType.DMA((4,))
    each = pltpu.SemaphoreType.DMA((sources,))
    return pl.pallas_call(
        functools.partial(tail_kernel, sources),
        out_shape=(
            jax.ShapeDtypeStruct(plane, jnp.float32),
            jax.ShapeDtypeStruct(plane, jnp.float32),
            jax.ShapeDtypeStruct((width // sources, channels), jnp.float32),
        ),
        in_specs=[pl.BlockSpec(memory_space=pltpu.VMEM)] * len(operands),
        out_specs=[pl.BlockSpec(memory_space=pltpu.VMEM)] * 3,
        scratch_shapes=[
            pltpu.VMEM((4, tokens, width // 4), jnp.bfloat16),
            pltpu.VMEM((tokens, width), jnp.bfloat16),
            pltpu.VMEM((sources, tokens, width // sources), jnp.bfloat16),
            pltpu.VMEM((sources, 8, channels), jnp.float32),
            pltpu.VMEM((sources, tokens, channels), jnp.bfloat16),
            pltpu.VMEM((tokens, 1), jnp.float32),
            pltpu.VMEM((8,) + plane, jnp.float32),
            pltpu.VMEM(plane, jnp.float32),
            pltpu.VMEM((2,) + plane, jnp.float32),
            pltpu.VMEM((2,) + plane, jnp.float32),
        ] + [four] * 6 + [each] * 12,
        compiler_params=pltpu.CompilerParams(collective_id=1, has_side_effects=True),
    )(*operands)


def body(
    out_grad,
    stream,
    norm_gain,
    routes,
    route_weight,
    gate_weight,
    up_weight,
    down_weight,
    out_proj,
    conv_out,
    gate_branch,
    decay_map,
    input_map,
    decay_param,
    decay_shift,
    states,
):
    sources = lax.axis_size("sp")
    experts = EXP_DEV * sources
    capacity = (5 * TOP * TOK_DEV + 4 * experts - 1) // (4 * experts)
    capacity = (capacity + 15) // 16 * 16
    row_grad, gate_grads, up_grads, down_grads = front(
        sources,
        capacity,
        stream,
        out_grad,
        norm_gain[None, :],
        routes.T,
        route_weight.T,
        gate_weight[0],
        up_weight[0],
        down_weight[0],
    )
    conv_grad, gate_branch_grad, out_proj_grad = tail(
        sources,
        row_grad,
        out_grad,
        stream,
        norm_gain[None, :],
        out_proj,
        conv_out,
        gate_branch,
        decay_map[:, 0],
        input_map[:, 0],
        decay_param,
        decay_shift,
        states,
    )
    gate_grads, up_grads, down_grads, conv_grad, gate_branch_grad, out_proj_grad = settle(
        gate_grads, up_grads, down_grads, conv_grad, gate_branch_grad, out_proj_grad
    )
    return (
        conv_grad,
        gate_branch_grad,
        out_proj_grad,
        gate_grads[None],
        up_grads[None],
        down_grads[None],
    )


def solution(mesh):
    placed = (
        P("sp", None),
        P("sp", None),
        P(),
        P("sp", None),
        P("sp", None),
        P("sp", None, "tp"),
        P("sp", None, "tp"),
        P("sp", "tp", None),
        P(None, "tp"),
        P("sp", "tp"),
        P("sp", "tp"),
        P(None, "tp", None, None),
        P(None, "tp", None, None),
        P(None, "tp"),
        P(None, "sp", "tp"),
        P(None, "sp", "tp"),
    )
    return jax.shard_map(
        body,
        mesh=mesh,
        in_specs=placed,
        out_specs=(
            P("sp", "tp"),
            P("sp", "tp"),
            P("sp", "tp"),
            P("sp", None, "tp"),
            P("sp", None, "tp"),
            P("sp", "tp", None),
        ),
        check_vma=False,
    )
```

```python
import functools

import jax
import jax.numpy as jnp
from jax import lax
from jax.experimental import pallas as pl
from jax.experimental.pallas import tpu as pltpu
from jax.sharding import PartitionSpec as P

TOP = 2
EXP_DEV = 1
TOK_DEV = 256


rate_scale = 8.0
norm_eps = 1e-06


def contract(left, right, left_dim, right_dim):
    return lax.dot_general(
        left, right, (((left_dim,), (right_dim,)), ((), ())), preferred_element_type=jnp.float32
    )


MESH = pl.DeviceIdType.MESH


def push(source, target, send_sem, recv_sem, where):
    return pltpu.make_async_remote_copy(
        src_ref=source,
        dst_ref=target,
        send_sem=send_sem,
        recv_sem=recv_sem,
        device_id=where,
        device_id_type=MESH,
    )


def loop(low, high, step):
    def one(index, carry):
        step(index)
        return carry

    lax.fori_loop(low, high, one, 0)


def partner(me, step, sources):
    total = jnp.int32(0)
    for place in range((sources - 1).bit_length()):
        weight = 1 << place
        left = lax.rem(lax.div(me, weight), 2)
        right = lax.rem(lax.div(step, weight), 2) if not isinstance(step, int) else step // weight % 2
        total = total + weight * (left + right - 2 * left * right)
    return total


def announce(sources, me, others):
    barrier = pltpu.get_barrier_semaphore()

    def one(step):
        pl.semaphore_signal(
            barrier, inc=1, device_id={"sp": lax.rem(me + step, sources)}, device_id_type=MESH
        )

    loop(1, sources, one)
    for other in others:
        pl.semaphore_signal(barrier, inc=1, device_id={"tp": other}, device_id_type=MESH)


def all_here(sources, others):
    pl.semaphore_wait(pltpu.get_barrier_semaphore(), sources - 1 + len(others))


def softplus(values):
    return jnp.maximum(values, 0.0) + jnp.log1p(jnp.exp(-jnp.abs(values)))


def minus_expm1(values):
    small = values * (1.0 / 5040.0)
    for divisor in (720.0, 120.0, 24.0, 6.0, 2.0, 1.0):
        small = (small + 1.0 / divisor) * values
    return jnp.where(values > -0.25, -small, 1.0 - jnp.exp(values))


def split_dot(values, maps):
    high = values.astype(jnp.bfloat16)
    rest = values - high.astype(jnp.float32)
    middle = rest.astype(jnp.bfloat16)
    low = (rest - middle.astype(jnp.float32)).astype(jnp.bfloat16)
    return contract(high, maps, 1, 1) + contract(middle, maps, 1, 1) + contract(low, maps, 1, 1)


def scan_rows(coeffs, values, reverse):
    rows = coeffs.shape[0]
    place = lax.broadcasted_iota(jnp.int32, coeffs.shape, 0)
    step = 1
    while step < rows:
        shift = rows - step if reverse else step
        inside = (place < rows - step) if reverse else (place >= step)
        moved_values = jnp.where(inside, pltpu.roll(values, shift, 0), 0.0)
        moved_coeffs = jnp.where(inside, pltpu.roll(coeffs, shift, 0), 1.0)
        values = values + coeffs * moved_values
        coeffs = coeffs * moved_coeffs
        step *= 2
    return coeffs, values


def front_kernel(
    sources, capacity, stream, out_grad, gain, routes, weights, gate_hbm, up_hbm, down_hbm,
    row_grad, gate_out, up_out, down_out,
    gate_w, up_w, down_w, gate_wg, up_wg, down_wg,
    place, slot_weight, normed, send_in, send_ct, rows_in, rows_ct, part, near, distant, back,
    hidden, pre_grad,
    load, store, send_a, recv_a, send_b, recv_b, send_c, recv_c, send_d, recv_d,
    send_n, recv_n, send_f, recv_f, send_h, recv_h
):
    me, mine = lax.axis_index("sp"), lax.axis_index("tp")
    beside = mine + 1 - 2 * lax.rem(mine, 2)
    across = lax.rem(mine + 2, 4)
    diagonal = lax.rem(beside + 2, 4)
    tokens, model = stream.shape
    width = model // 4
    units = gate_w.shape[1]
    slots = sources * capacity
    announce(sources, me, (beside, across))
    loads = [
        pltpu.make_async_copy(src, dst, load.at[index])
        for index, (src, dst) in enumerate(((gate_hbm, gate_w), (up_hbm, up_w), (down_hbm, down_w)))
    ]
    for copy in loads:
        copy.start()

    def columns(which):
        return pl.ds(pl.multiple_of(which * width, width), width)

    def rows_of(slot):
        return pl.ds(pl.multiple_of(slot * capacity, capacity), capacity)

    expert = lax.broadcasted_iota(jnp.int32, (128, tokens), 0)
    chosen = jnp.where((routes[0:1] == expert) | (routes[1:2] == expert), 1.0, 0.0).astype(
        jnp.bfloat16
    )
    earlier = lax.broadcasted_iota(jnp.int32, (tokens, tokens), 0) < lax.broadcasted_iota(
        jnp.int32, (tokens, tokens), 1
    )
    rank = contract(chosen, jnp.where(earlier, 1.0, 0.0).astype(jnp.bfloat16), 1, 0).astype(
        jnp.bfloat16
    )
    slot_row = lax.broadcasted_iota(jnp.int32, (slots, 128), 0)
    slot_lane = lax.broadcasted_iota(jnp.int32, (slots, 128), 1)
    slot_low = slot_lane * capacity
    owner = (slot_row >= slot_low) & (slot_row < slot_low + capacity)
    named = jnp.sum(jnp.where(owner, slot_lane.astype(jnp.float32), 0.0), axis=1, keepdims=True)
    offset = jnp.sum(
        jnp.where(owner, (slot_row - slot_low).astype(jnp.float32), 0.0), axis=1, keepdims=True
    )
    ranks = contract(jnp.where(owner, 1.0, 0.0).astype(jnp.bfloat16), rank, 1, 0)
    fits = ranks == offset
    first_is = (routes[0:1].astype(jnp.float32) == named) & fits
    second_is = (routes[1:2].astype(jnp.float32) == named) & fits
    place[...] = jnp.where(first_is | second_is, 1.0, 0.0).astype(jnp.bfloat16)
    slot_weight[...] = jnp.sum(
        jnp.where(first_is, weights[0:1], 0.0) + jnp.where(second_is, weights[1:2], 0.0),
        axis=1, keepdims=True,
    )

    def norm_rows(index):
        view = pl.ds(pl.multiple_of(index * 16, 16), 16)
        total = jnp.zeros((16, 1), jnp.float32)
        for q in range(4):
            values = stream[view, q * width : (q + 1) * width].astype(jnp.float32)
            total = total + jnp.sum(values * values, axis=1, keepdims=True)
        row_scale = lax.rsqrt(total / model + norm_eps)
        for q in range(4):
            run = slice(q * width, (q + 1) * width)
            normed[view, run] = (
                stream[view, run].astype(jnp.float32) * row_scale * gain[run].astype(jnp.float32)[None, :]
            ).astype(jnp.bfloat16)

    all_here(sources, (beside, across))
    pairs = ((send_in, rows_in), (send_ct, rows_ct))

    def first(arr, step, slot, quarter, owner_slot):
        src, dst = pairs[arr]
        return push(
            src.at[slot], dst.at[rows_of(owner_slot), columns(quarter)],
            send_a.at[arr, slot], recv_a.at[arr, slot], {"sp": partner(me, step, sources)},
        )

    def give_ct(step, slot, quarter):
        view = rows_of(partner(me, step, sources))
        send_ct[slot] = (
            slot_weight[view] * contract(place[view], out_grad[:, columns(quarter)], 1, 0)
        ).astype(jnp.bfloat16)
        first(1, step, slot, quarter, me).start()

    def give_in(step, slot, quarter):
        view = rows_of(partner(me, step, sources))
        send_in[slot] = contract(place[view], normed[:, columns(quarter)], 1, 0).astype(
            jnp.bfloat16
        )
        first(0, step, slot, quarter, me).start()

    def give(step):
        give_ct(step, step, mine)
        give_in(step, step, mine)

    half = sources // 2
    place_z = lax.div(me * 4, sources)
    at_end = (place_z == 0) | (place_z == 3)

    def nth(index):
        return 2 + lax.rem(index + half - 2, sources - 2)

    def give_second(step):
        give_ct(step, sources - 1 + step, across)
        give_in(step, sources - 1 + step, across)

    give_ct(1, 1, mine)
    give_ct(nth(0), nth(0), mine)
    loop(0, tokens // 16, norm_rows)
    give_in(1, 1, mine)
    give_in(nth(0), nth(0), mine)

    loop(1, sources - 2, lambda index: give(nth(index)))
    loop(2, 4, give_second)
    give_second(1)
    own = rows_of(me)

    def own_columns(quarter):
        picked = place[own]
        rows_in[own, columns(quarter)] = contract(picked, normed[:, columns(quarter)], 1, 0).astype(
            jnp.bfloat16
        )
        rows_ct[own, columns(quarter)] = (
            slot_weight[own] * contract(picked, out_grad[:, columns(quarter)], 1, 0)
        ).astype(jnp.bfloat16)

    loop(0, 4, own_columns)

    def passed(arr, step, quarter, send, recv, target):
        view = pairs[arr][1].at[rows_of(partner(me, step, sources)), columns(quarter)]
        return push(view, view, send.at[arr, step], recv.at[arr, step], {"tp": target})

    def relay(step):
        slot = partner(me, step, sources)
        for arr in range(2):
            first(arr, step, step, mine, slot).wait_recv()
            passed(arr, step, mine, send_c, recv_c, across).start()
            passed(arr, step, mine, send_b, recv_b, beside).start()

    def onward(step):
        for arr in range(2):
            passed(arr, step, across, send_c, recv_c, across).wait_recv()
            passed(arr, step, across, send_d, recv_d, beside).start()

    def complete(step):
        for arr in range(2):
            passed(arr, step, beside, send_b, recv_b, beside).wait_recv()
            passed(arr, step, diagonal, send_d, recv_d, beside).wait_recv()

    def compute(step):
        view = rows_of(partner(me, step, sources))
        inputs = rows_in[view]
        gate_pre = contract(inputs, gate_w[...], 1, 0)
        up_pre = contract(inputs, up_w[...], 1, 0)
        logistic = jax.nn.sigmoid(gate_pre)
        gated = gate_pre * logistic
        hidden[view] = (gated * up_pre).astype(jnp.bfloat16)
        hidden_grad = contract(rows_ct[view], down_w[...], 1, 1)
        up_grad = (hidden_grad * gated).astype(jnp.bfloat16)
        gate_grad = (
            hidden_grad * up_pre * (logistic * (1.0 + gate_pre * (1.0 - logistic)))
        ).astype(jnp.bfloat16)
        pre_grad[view, :units] = gate_grad
        pre_grad[view, units:] = up_grad

        def back_columns(quarter):
            rows = columns(quarter)
            part[view, rows] = (
                contract(gate_grad, gate_w[rows], 1, 1) + contract(up_grad, up_w[rows], 1, 1)
            ).astype(jnp.bfloat16)

        loop(0, 4, back_columns)

    def part_of(step, quarter):
        return part[rows_of(partner(me, step, sources)), columns(quarter)].astype(jnp.float32)

    def near_copy(step, half, quarter):
        return push(
            part.at[rows_of(partner(me, step, sources)), columns(quarter)], near.at[step, half],
            send_n.at[step, half], recv_n.at[step, half], {"tp": beside},
        )

    def far_copy(step):
        return push(
            send_in.at[step], distant.at[step], send_f.at[step], recv_f.at[step], {"tp": across}
        )

    def home_copy(step, slot):
        return push(
            send_ct.at[step], back.at[rows_of(slot)], send_h.at[step], recv_h.at[step],
            {"sp": partner(me, step, sources)},
        )

    def share_near(step):
        near_copy(step, 1, diagonal).start()
        near_copy(step, 0, beside).start()

    def share_far(step):
        near_copy(step, 1, diagonal).wait_recv()

        @pl.when(step > 0)
        def _():
            first(0, step, step, mine, me).wait_send()

        send_in[step] = (part_of(step, across) + near[step, 1].astype(jnp.float32)).astype(
            jnp.bfloat16
        )
        far_copy(step).start()

    def send_home(step):
        near_copy(step, 0, beside).wait_recv()
        far_copy(step).wait_recv()
        total = (
            part_of(step, mine)
            + near[step, 0].astype(jnp.float32)
            + distant[step].astype(jnp.float32)
        ).astype(jnp.bfloat16)

        @pl.when(step > 0)
        def _():
            first(1, step, step, mine, me).wait_send()
            send_ct[step] = total
            home_copy(step, me).start()

        @pl.when(step == 0)
        def _():
            back[own] = total

    for copy in loads:
        copy.wait()

    def turn(index):
        early = jnp.where(at_end, sources - 2, half)
        late = jnp.where(at_end | (index < half), index, index + 2)
        step = jnp.where(index < 2, 1, jnp.where(index < 4, early + index - 2, jnp.where(index < sources - 2, late, index - sources + 4)))
        return jnp.where(index == 0, 0, step)

    def relay_turn(index):
        step = turn(index)

        @pl.when(step < 4)
        def _():
            slot = partner(me, step, sources)
            for arr in range(2):
                first(arr, step, step, mine, slot).wait_recv()
                passed(arr, step, mine, send_b, recv_b, beside).start()
            for arr in range(2):
                first(arr, step, sources - 1 + step, across, slot).wait_recv()
                passed(arr, step, across, send_d, recv_d, beside).start()

        @pl.when(step > 3)
        def _():
            relay(step)

    def onward_turn(index):
        @pl.when(turn(index) > 3)
        def _():
            onward(turn(index))

    def stage(index):
        step = turn(index)

        @pl.when(index > 0)
        def _():
            complete(step)

        compute(step)
        share_near(step)
        share_far(step)

        @pl.when(index == 0)
        def _():
            relay_turn(1)

        @pl.when(index + 2 < sources)
        def _():
            relay_turn(index + 2)

        @pl.when(index + 1 < sources)
        def _():
            onward_turn(index + 1)

        @pl.when(index > 0)
        def _():
            send_home(turn(index - 1))

    loop(0, sources, stage)
    run = model // 8

    def stored(index):
        view = pl.ds(pl.multiple_of(index * run, run), run)
        return [
            pltpu.make_async_copy(src.at[where], dst.at[where], store.at[arr, index])
            for arr, (src, dst, where) in enumerate(
                ((gate_wg, gate_out, view), (up_wg, up_out, view), (down_wg, down_out, (slice(None), view)))
            )
        ]

    def weight_run(index):
        view = pl.ds(pl.multiple_of(index * run, run), run)
        both = contract(rows_in[:, view], pre_grad[...], 0, 0).astype(jnp.bfloat16)
        gate_wg[view] = both[:, :units]
        up_wg[view] = both[:, units:]
        down_wg[:, view] = contract(hidden[...], rows_ct[:, view], 0, 0).astype(jnp.bfloat16)
        for copy in stored(index):
            copy.start()

    loop(0, 5, weight_run)
    send_home(turn(sources - 1))
    loop(5, 8, weight_run)

    def finish_home(step):
        home_copy(step, partner(me, step, sources)).wait_recv()

    loop(1, sources, finish_home)
    row_grad[...] = contract(place[...], back[...], 0, 0).astype(jnp.bfloat16)

    def finish_sends(step):
        near_copy(step, 0, beside).wait_send()
        near_copy(step, 1, diagonal).wait_send()
        far_copy(step).wait_send()

        @pl.when(step > 0)
        def _():
            home_copy(step, me).wait_send()
            for arr in range(2):
                passed(arr, step, mine, send_b, recv_b, beside).wait_send()
                passed(arr, step, across, send_d, recv_d, beside).wait_send()

        @pl.when(step > 3)
        def _():
            for arr in range(2):
                passed(arr, step, mine, send_c, recv_c, across).wait_send()

    loop(0, sources, finish_sends)
    for step in range(1, 4):
        for arr in range(2):
            first(arr, step, sources - 1 + step, across, me).wait_send()

    def finish_stores(index):
        for copy in stored(index):
            copy.wait()

    loop(0, 8, finish_stores)


def front(sources, capacity, *operands):
    stream, gate_weight, down_weight = operands[0], operands[5], operands[7]
    tokens, model = stream.shape
    units = gate_weight.shape[1]
    slots, width = sources * capacity, model // 4
    narrow = jnp.bfloat16
    vmem, anywhere = pl.BlockSpec(memory_space=pltpu.VMEM), pl.BlockSpec(memory_space=pl.ANY)
    tall, wide = gate_weight.shape, down_weight.shape
    dma = pltpu.SemaphoreType.DMA
    return pl.pallas_call(
        functools.partial(front_kernel, sources, capacity),
        out_shape=(
            jax.ShapeDtypeStruct((tokens, width), narrow),
            jax.ShapeDtypeStruct(tall, narrow),
            jax.ShapeDtypeStruct(tall, narrow),
            jax.ShapeDtypeStruct(wide, narrow),
        ),
        in_specs=[vmem] * 5 + [anywhere] * 3,
        out_specs=[vmem] + [anywhere] * 3,
        scratch_shapes=[
            pltpu.VMEM(tall, narrow), pltpu.VMEM(tall, narrow), pltpu.VMEM(wide, narrow),
            pltpu.VMEM(tall, narrow), pltpu.VMEM(tall, narrow), pltpu.VMEM(wide, narrow),
            pltpu.VMEM((slots, tokens), narrow),
            pltpu.VMEM((slots, 1), jnp.float32),
            pltpu.VMEM((tokens, model), narrow),
            pltpu.VMEM((sources + 3, capacity, width), narrow),
            pltpu.VMEM((sources + 3, capacity, width), narrow),
            pltpu.VMEM((slots, model), narrow),
            pltpu.VMEM((slots, model), narrow),
            pltpu.VMEM((slots, model), narrow),
            pltpu.VMEM((sources, 2, capacity, width), narrow),
            pltpu.VMEM((sources, capacity, width), narrow),
            pltpu.VMEM((slots, width), narrow),
            pltpu.VMEM((slots, units), narrow),
            pltpu.VMEM((slots, 2 * units), narrow),
            dma((3,)), dma((3, 8)), dma((2, sources + 3)), dma((2, sources + 3)),
        ] + [dma((2, sources))] * 6 + [dma((sources, 2))] * 2 + [dma((sources,))] * 4,
        compiler_params=pltpu.CompilerParams(
            collective_id=0, has_side_effects=True, vmem_limit_bytes=67043328
        ),
    )(*operands)


def settle_kernel(*refs):
    count = (len(refs) - 2) // 3
    load, store = refs[-2:]
    loads = [pltpu.make_async_copy(refs[i], refs[2 * count + i], load.at[i]) for i in range(count)]
    stores = [
        pltpu.make_async_copy(refs[2 * count + i], refs[count + i], store.at[i])
        for i in range(count)
    ]
    for copy in loads:
        copy.start()
    for before, after in zip(loads, stores):
        before.wait()
        after.start()
    for copy in stores:
        copy.wait()


def settle(*arrays):
    anywhere = pl.BlockSpec(memory_space=pl.ANY)
    dma = pltpu.SemaphoreType.DMA((len(arrays),))
    return pl.pallas_call(
        settle_kernel,
        out_shape=tuple(jax.ShapeDtypeStruct(a.shape, a.dtype) for a in arrays),
        in_specs=[anywhere] * len(arrays),
        out_specs=[anywhere] * len(arrays),
        scratch_shapes=[pltpu.VMEM(a.shape, a.dtype) for a in arrays] + [dma, dma],
    )(*arrays)


def tail_kernel(
    sources, row_grad, out_grad, stream, gain, out_proj, conv, branch, dmap, imap,
    dparam, dshift, states, conv_grad, branch_grad, proj_grad,
    normed_grad, grad_b, rows, sums, lru, scale, gates, state_grad, reach, inner,
    send_x, recv_x, send_b, recv_b, send_d, recv_d,
    send_p, recv_p, send_px, recv_px, send_pb, recv_pb, send_pd, recv_pd, send_s, recv_s,
    send_l, recv_l
):
    me, mine = lax.axis_index("sp"), lax.axis_index("tp")
    beside = mine + 1 - 2 * lax.rem(mine, 2)
    across = lax.rem(mine + 2, 4)
    diagonal = lax.rem(beside + 2, 4)
    tokens, width = out_grad.shape
    quarter = width // 4
    chunk = tokens // 4
    piece = width // sources
    channels = conv.shape[1]
    announce(sources, me, (beside, across))
    normed_grad[mine] = row_grad[...]
    gate = branch[...].astype(jnp.float32)
    slope = 0.7978845608028654
    inside = jnp.tanh(slope * (gate + 0.044715 * gate * gate * gate))
    lru[me] = ((states[0] + states[1]) * (0.5 * gate * (1.0 + inside))).astype(jnp.bfloat16)
    all_here(sources, (beside, across))

    def part(which, index, send, recv, target):
        view = normed_grad.at[which, pl.ds(index * chunk, chunk)]
        return push(view, view, send.at[index], recv.at[index], {"tp": target})

    for index in range(4):
        part(mine, index, send_x, recv_x, across).start()
        part(mine, index, send_b, recv_b, beside).start()

    def lru_copy(step, slot):
        return push(
            lru.at[slot], lru.at[slot], send_l.at[step], recv_l.at[step],
            {"sp": partner(me, step, sources)},
        )

    half = sources // 2
    early = half + (3 * half) // 4
    lru_copy(1, me).start()
    loop(half, early, lambda step: lru_copy(step, me).start())

    def squares(index):
        low = pl.multiple_of(index * 16, 16)
        total = jnp.zeros((16, 1), jnp.float32)
        for q in range(4):
            values = stream[pl.ds(low, 16), q * quarter : (q + 1) * quarter].astype(jnp.float32)
            total = total + jnp.sum(values * values, axis=1, keepdims=True)
        scale[pl.ds(low, 16)] = lax.rsqrt(total / width + norm_eps)

    loop(0, tokens // 16, squares)

    def relay_part(index):
        part(across, index, send_x, recv_x, across).wait_recv()
        part(across, index, send_d, recv_d, beside).start()

    block = 64
    for direction in range(2):
        relay_part(2 * direction)
        base = softplus(-dparam[direction : direction + 1])
        def gate_rows(index):
            low = pl.multiple_of(index * block, block)
            view = pl.ds(low, block)
            held = conv[view]
            decay_gate = jax.nn.sigmoid(contract(held, dmap[direction], 1, 0))
            input_gate = jax.nn.sigmoid(contract(held, imap[direction], 1, 0))
            log_decay = -rate_scale * decay_gate * base + dshift[direction, view]
            gates[4 * direction, view] = decay_gate
            gates[4 * direction + 1, view] = input_gate
            gates[4 * direction + 2, view] = jnp.exp(log_decay)
            gates[4 * direction + 3, view] = jnp.sqrt(minus_expm1(2.0 * log_decay))
        loop(0, tokens // block, gate_rows)
        relay_part(2 * direction + 1)

    def piece_copy(step):
        peer = partner(me, step, sources)
        return push(
            grad_b.at[pl.ds(pl.multiple_of(mine * chunk, chunk), chunk), pl.ds(pl.multiple_of(peer * piece, piece), piece)],
            rows.at[me, pl.ds(pl.multiple_of(mine * chunk, chunk), chunk)],
            send_p.at[step], recv_p.at[step], {"sp": peer},
        )

    def piece_landed(step):
        peer = partner(me, step, sources)
        return push(
            grad_b.at[pl.ds(pl.multiple_of(mine * chunk, chunk), chunk), pl.ds(pl.multiple_of(me * piece, piece), piece)],
            rows.at[peer, pl.ds(pl.multiple_of(mine * chunk, chunk), chunk)],
            send_p.at[step], recv_p.at[step], {"sp": peer},
        )

    def piece_pass(step, which, send, recv, target):
        view = rows.at[partner(me, step, sources), pl.ds(pl.multiple_of(which * chunk, chunk), chunk)]
        return push(view, view, send.at[step], recv.at[step], {"tp": target})

    for index in range(4):
        part(beside, index, send_b, recv_b, beside).wait_recv()
        part(diagonal, index, send_d, recv_d, beside).wait_recv()

        def grad_rows(inside):
            low = pl.multiple_of(index * chunk + inside * 16, 16)
            view = pl.ds(low, 16)
            own_scale = scale[view]
            total = jnp.zeros((16, 1), jnp.float32)
            for q in range(4):
                run = slice(q * quarter, (q + 1) * quarter)
                scaled = gain[run].astype(jnp.float32)[None, :] * normed_grad[q, view].astype(jnp.float32)
                total = total + jnp.sum(
                    stream[view, run].astype(jnp.float32) * scaled, axis=1, keepdims=True
                )
            factor = own_scale * own_scale * total / width
            for q in range(4):
                run = slice(q * quarter, (q + 1) * quarter)
                scaled = gain[run].astype(jnp.float32)[None, :] * normed_grad[q, view].astype(jnp.float32)
                grad_b[view, run] = (
                    out_grad[view, run].astype(jnp.float32)
                    + own_scale * (scaled - stream[view, run].astype(jnp.float32) * factor)
                ).astype(jnp.bfloat16)

        loop(0, chunk // 16, grad_rows)

        @pl.when(mine == index)
        def _():
            loop(1, sources, lambda step: piece_copy(sources - step).start())

    lru_out_grad = contract(grad_b[...], out_proj[...], 1, 0)
    gate = branch[...].astype(jnp.float32)
    slope = 0.7978845608028654
    inside = jnp.tanh(slope * (gate + 0.044715 * gate * gate * gate))
    gelu_gate = 0.5 * gate * (1.0 + inside)
    gelu_slope = 0.5 * (1.0 + inside) + 0.5 * gate * (1.0 - inside * inside) * slope * (
        1.0 + 3.0 * 0.044715 * gate * gate
    )
    branch_grad[...] = lru_out_grad * (states[0] + states[1]) * gelu_slope
    state_grad[...] = lru_out_grad * gelu_gate

    def relay(step):
        piece_landed(step).wait_recv()
        piece_pass(step, mine, send_px, recv_px, across).start()
        piece_pass(step, mine, send_pb, recv_pb, beside).start()

    def onward(step):
        piece_pass(step, across, send_px, recv_px, across).wait_recv()
        piece_pass(step, across, send_pd, recv_pd, beside).start()

    place = lax.broadcasted_iota(jnp.int32, (tokens, channels), 0)
    for direction in range(2):
        decay = gates[4 * direction + 2]
        if direction == 0:
            coeffs = jnp.where(place < tokens - 1, pltpu.roll(decay, tokens - 1, 0), 1.0)
            edge = 0
        else:
            coeffs = jnp.where(place >= 1, pltpu.roll(decay, 1, 0), 1.0)
            edge = tokens - 1
        coeffs, values = scan_rows(coeffs, state_grad[...], direction == 0)
        reach[direction] = coeffs
        inner[direction] = values
        edge_decay = decay[edge : edge + 1]
        sums[me, 2 * direction : 2 * direction + 1] = edge_decay * coeffs[edge : edge + 1]
        sums[me, 2 * direction + 1 : 2 * direction + 2] = edge_decay * values[edge : edge + 1]

    def sums_copy(step, slot):
        return push(
            sums.at[slot], sums.at[slot], send_s.at[step], recv_s.at[step],
            {"sp": partner(me, step, sources)},
        )

    loop(1, sources, lambda step: sums_copy(sources - step, me).start())
    loop(early, sources, lambda step: lru_copy(step, me).start())
    loop(2, half, lambda step: lru_copy(step, me).start())
    loop(1, half, relay)
    loop(1, half, onward)
    loop(half, sources, relay)
    loop(1, sources, lambda step: sums_copy(step, partner(me, step, sources)).wait_recv())
    zero_row = jnp.zeros((1, channels), jnp.float32)

    def from_right(index, carry):
        slot = sources - 1 - index
        ours = sums[slot, 0:1] * carry + sums[slot, 1:2]
        return jnp.where(slot > me, ours, carry)

    def from_left(slot, carry):
        ours = sums[slot, 2:3] * carry + sums[slot, 3:4]
        return jnp.where(slot < me, ours, carry)

    incoming = (
        lax.fori_loop(0, sources, from_right, zero_row),
        lax.fori_loop(0, sources, from_left, zero_row),
    )
    for direction in range(2):
        base = softplus(-dparam[direction : direction + 1])

        def back_rows(index):
            view = pl.ds(pl.multiple_of(index * block, block), block)
            decay_gate, input_gate = gates[4 * direction, view], gates[4 * direction + 1, view]
            decay_rate, drive_scale = gates[4 * direction + 2, view], gates[4 * direction + 3, view]
            conv_float = conv[view].astype(jnp.float32)
            adjoint = inner[direction, view] + reach[direction, view] * incoming[direction]
            driven = input_gate * conv_float
            log_grad = adjoint * (
                states[direction, view] - drive_scale * driven
                - driven * decay_rate * decay_rate / drive_scale
            )
            decay_pre_grad = log_grad * (-rate_scale * base) * decay_gate * (1.0 - decay_gate)
            input_pre_grad = adjoint * drive_scale * driven * (1.0 - input_gate)
            ours = (
                adjoint * drive_scale * input_gate
                + split_dot(decay_pre_grad, dmap[direction])
                + split_dot(input_pre_grad, imap[direction])
            )
            conv_grad[view] = ours if direction == 0 else conv_grad[view] + ours

        loop(0, tokens // block, back_rows)
    loop(half, sources, onward)
    proj_grad[...] = contract(
        grad_b[:, pl.ds(pl.multiple_of(me * piece, piece), piece)], lru[me], 0, 0
    )

    def gather_product(step):
        slot = partner(me, step, sources)
        lru_copy(step, slot).wait_recv()
        piece_pass(step, beside, send_pb, recv_pb, beside).wait_recv()
        piece_pass(step, diagonal, send_pd, recv_pd, beside).wait_recv()
        proj_grad[...] += contract(rows[slot], lru[slot], 0, 0)

    loop(1, sources, gather_product)

    def finish(step):
        piece_copy(step).wait_send()
        piece_pass(step, mine, send_px, recv_px, across).wait_send()
        piece_pass(step, mine, send_pb, recv_pb, beside).wait_send()
        piece_pass(step, across, send_pd, recv_pd, beside).wait_send()
        sums_copy(step, me).wait_send()
        lru_copy(step, me).wait_send()

    loop(1, sources, finish)
    for index in range(4):
        part(mine, index, send_x, recv_x, across).wait_send()
        part(mine, index, send_b, recv_b, beside).wait_send()
        part(across, index, send_d, recv_d, beside).wait_send()


def tail(sources, *operands):
    out_grad, conv = operands[1], operands[5]
    tokens, width = out_grad.shape
    channels = conv.shape[1]
    plane = (tokens, channels)
    four = pltpu.SemaphoreType.DMA((4,))
    each = pltpu.SemaphoreType.DMA((sources,))
    return pl.pallas_call(
        functools.partial(tail_kernel, sources),
        out_shape=(
            jax.ShapeDtypeStruct(plane, jnp.float32),
            jax.ShapeDtypeStruct(plane, jnp.float32),
            jax.ShapeDtypeStruct((width // sources, channels), jnp.float32),
        ),
        in_specs=[pl.BlockSpec(memory_space=pltpu.VMEM)] * len(operands),
        out_specs=[pl.BlockSpec(memory_space=pltpu.VMEM)] * 3,
        scratch_shapes=[
            pltpu.VMEM((4, tokens, width // 4), jnp.bfloat16),
            pltpu.VMEM((tokens, width), jnp.bfloat16),
            pltpu.VMEM((sources, tokens, width // sources), jnp.bfloat16),
            pltpu.VMEM((sources, 8, channels), jnp.float32),
            pltpu.VMEM((sources, tokens, channels), jnp.bfloat16),
            pltpu.VMEM((tokens, 1), jnp.float32),
            pltpu.VMEM((8,) + plane, jnp.float32),
            pltpu.VMEM(plane, jnp.float32),
            pltpu.VMEM((2,) + plane, jnp.float32),
            pltpu.VMEM((2,) + plane, jnp.float32),
        ] + [four] * 6 + [each] * 12,
        compiler_params=pltpu.CompilerParams(collective_id=1, has_side_effects=True),
    )(*operands)


def body(
    out_grad,
    stream,
    norm_gain,
    routes,
    route_weight,
    gate_weight,
    up_weight,
    down_weight,
    out_proj,
    conv_out,
    gate_branch,
    decay_map,
    input_map,
    decay_param,
    decay_shift,
    states,
):
    sources = lax.axis_size("sp")
    experts = EXP_DEV * sources
    capacity = (5 * TOP * TOK_DEV + 4 * experts - 1) // (4 * experts)
    capacity = (capacity + 15) // 16 * 16
    row_grad, gate_grads, up_grads, down_grads = front(
        sources,
        capacity,
        stream,
        out_grad,
        norm_gain,
        routes.T,
        route_weight.T,
        gate_weight[0],
        up_weight[0],
        down_weight[0],
    )
    conv_grad, gate_branch_grad, out_proj_grad = tail(
        sources,
        row_grad,
        out_grad,
        stream,
        norm_gain,
        out_proj,
        conv_out,
        gate_branch,
        decay_map[:, 0],
        input_map[:, 0],
        decay_param,
        decay_shift,
        states,
    )
    gate_grads, up_grads, down_grads, conv_grad, gate_branch_grad, out_proj_grad = settle(
        gate_grads, up_grads, down_grads, conv_grad, gate_branch_grad, out_proj_grad
    )
    return (
        conv_grad,
        gate_branch_grad,
        out_proj_grad,
        gate_grads[None],
        up_grads[None],
        down_grads[None],
    )


def solution(mesh):
    placed = (
        P("sp", None),
        P("sp", None),
        P(),
        P("sp", None),
        P("sp", None),
        P("sp", None, "tp"),
        P("sp", None, "tp"),
        P("sp", "tp", None),
        P(None, "tp"),
        P("sp", "tp"),
        P("sp", "tp"),
        P(None, "tp", None, None),
        P(None, "tp", None, None),
        P(None, "tp"),
        P(None, "sp", "tp"),
        P(None, "sp", "tp"),
    )
    return jax.shard_map(
        body,
        mesh=mesh,
        in_specs=placed,
        out_specs=(
            P("sp", "tp"),
            P("sp", "tp"),
            P("sp", "tp"),
            P("sp", None, "tp"),
            P("sp", None, "tp"),
            P("sp", "tp", None),
        ),
        check_vma=False,
    )
```

```python
import functools

import jax
import jax.numpy as jnp
from jax import lax
from jax.experimental import pallas as pl
from jax.experimental.pallas import tpu as pltpu
from jax.sharding import PartitionSpec as P

TOP = 2
EXP_DEV = 1
TOK_DEV = 256


rate_scale = 8.0
norm_eps = 1e-06


def contract(left, right, left_dim, right_dim):
    return lax.dot_general(
        left, right, (((left_dim,), (right_dim,)), ((), ())), preferred_element_type=jnp.float32
    )


MESH = pl.DeviceIdType.MESH


def push(source, target, send_sem, recv_sem, where):
    return pltpu.make_async_remote_copy(
        src_ref=source,
        dst_ref=target,
        send_sem=send_sem,
        recv_sem=recv_sem,
        device_id=where,
        device_id_type=MESH,
    )


def loop(low, high, step):
    def one(index, carry):
        step(index)
        return carry

    lax.fori_loop(low, high, one, 0)


def partner(me, step, sources):
    total = jnp.int32(0)
    for place in range((sources - 1).bit_length()):
        weight = 1 << place
        left = lax.rem(lax.div(me, weight), 2)
        right = lax.rem(lax.div(step, weight), 2) if not isinstance(step, int) else step // weight % 2
        total = total + weight * (left + right - 2 * left * right)
    return total


def announce(sources, me, others):
    barrier = pltpu.get_barrier_semaphore()

    def one(step):
        pl.semaphore_signal(
            barrier, inc=1, device_id={"sp": lax.rem(me + step, sources)}, device_id_type=MESH
        )

    loop(1, sources, one)
    for other in others:
        pl.semaphore_signal(barrier, inc=1, device_id={"tp": other}, device_id_type=MESH)


def all_here(sources, others):
    pl.semaphore_wait(pltpu.get_barrier_semaphore(), sources - 1 + len(others))


def softplus(values):
    return jnp.maximum(values, 0.0) + jnp.log1p(jnp.exp(-jnp.abs(values)))


def minus_expm1(values):
    small = values * (1.0 / 5040.0)
    for divisor in (720.0, 120.0, 24.0, 6.0, 2.0, 1.0):
        small = (small + 1.0 / divisor) * values
    return jnp.where(values > -0.25, -small, 1.0 - jnp.exp(values))


def split_dot(values, maps):
    high = values.astype(jnp.bfloat16)
    rest = values - high.astype(jnp.float32)
    middle = rest.astype(jnp.bfloat16)
    low = (rest - middle.astype(jnp.float32)).astype(jnp.bfloat16)
    return contract(high, maps, 1, 1) + contract(middle, maps, 1, 1) + contract(low, maps, 1, 1)


def scan_rows(coeffs, values, reverse):
    rows = coeffs.shape[0]
    place = lax.broadcasted_iota(jnp.int32, coeffs.shape, 0)
    step = 1
    while step < rows:
        shift = rows - step if reverse else step
        inside = (place < rows - step) if reverse else (place >= step)
        moved_values = jnp.where(inside, pltpu.roll(values, shift, 0), 0.0)
        moved_coeffs = jnp.where(inside, pltpu.roll(coeffs, shift, 0), 1.0)
        values = values + coeffs * moved_values
        coeffs = coeffs * moved_coeffs
        step *= 2
    return coeffs, values


def front_kernel(
    sources, capacity, stream_hbm, out_hbm, gain, routes, weights, gate_hbm, up_hbm, down_hbm,
    row_grad, gate_out, up_out, down_out,
    stream, out_grad, gate_w, up_w, down_w, gate_wg, up_wg, down_wg,
    place, slot_weight, normed, send_in, send_ct, rows_in, rows_ct, part, near, distant, back,
    hidden, pre_grad,
    load, store, send_a, recv_a, send_b, recv_b, send_c, recv_c, send_d, recv_d,
    send_n, recv_n, send_f, recv_f, send_h, recv_h
):
    me, mine = lax.axis_index("sp"), lax.axis_index("tp")
    beside = mine + 1 - 2 * lax.rem(mine, 2)
    across = lax.rem(mine + 2, 4)
    diagonal = lax.rem(beside + 2, 4)
    tokens, model = stream.shape
    width = model // 4
    units = gate_w.shape[1]
    slots = sources * capacity
    announce(sources, me, (beside, across))
    loads = [
        pltpu.make_async_copy(src, dst, load.at[index])
        for index, (src, dst) in enumerate(
            ((out_hbm, out_grad), (stream_hbm, stream), (gate_hbm, gate_w), (up_hbm, up_w), (down_hbm, down_w))
        )
    ]
    for copy in loads:
        copy.start()

    def columns(which):
        return pl.ds(pl.multiple_of(which * width, width), width)

    def rows_of(slot):
        return pl.ds(pl.multiple_of(slot * capacity, capacity), capacity)

    expert = lax.broadcasted_iota(jnp.int32, (128, tokens), 0)
    chosen = jnp.where((routes[0:1] == expert) | (routes[1:2] == expert), 1.0, 0.0).astype(
        jnp.bfloat16
    )
    earlier = lax.broadcasted_iota(jnp.int32, (tokens, tokens), 0) < lax.broadcasted_iota(
        jnp.int32, (tokens, tokens), 1
    )
    rank = contract(chosen, jnp.where(earlier, 1.0, 0.0).astype(jnp.bfloat16), 1, 0).astype(
        jnp.bfloat16
    )
    slot_row = lax.broadcasted_iota(jnp.int32, (slots, 128), 0)
    slot_lane = lax.broadcasted_iota(jnp.int32, (slots, 128), 1)
    slot_low = slot_lane * capacity
    owner = (slot_row >= slot_low) & (slot_row < slot_low + capacity)
    named = jnp.sum(jnp.where(owner, slot_lane.astype(jnp.float32), 0.0), axis=1, keepdims=True)
    offset = jnp.sum(
        jnp.where(owner, (slot_row - slot_low).astype(jnp.float32), 0.0), axis=1, keepdims=True
    )
    ranks = contract(jnp.where(owner, 1.0, 0.0).astype(jnp.bfloat16), rank, 1, 0)
    fits = ranks == offset
    first_is = (routes[0:1].astype(jnp.float32) == named) & fits
    second_is = (routes[1:2].astype(jnp.float32) == named) & fits
    place[...] = jnp.where(first_is | second_is, 1.0, 0.0).astype(jnp.bfloat16)
    slot_weight[...] = jnp.sum(
        jnp.where(first_is, weights[0:1], 0.0) + jnp.where(second_is, weights[1:2], 0.0),
        axis=1, keepdims=True,
    )

    def norm_rows(index):
        view = pl.ds(pl.multiple_of(index * 16, 16), 16)
        total = jnp.zeros((16, 1), jnp.float32)
        for q in range(4):
            values = stream[view, q * width : (q + 1) * width].astype(jnp.float32)
            total = total + jnp.sum(values * values, axis=1, keepdims=True)
        row_scale = lax.rsqrt(total / model + norm_eps)
        for q in range(4):
            run = slice(q * width, (q + 1) * width)
            normed[view, run] = (
                stream[view, run].astype(jnp.float32) * row_scale * gain[run].astype(jnp.float32)[None, :]
            ).astype(jnp.bfloat16)

    all_here(sources, (beside, across))
    loads[0].wait()
    pairs = ((send_in, rows_in), (send_ct, rows_ct))

    def first(arr, step, slot, quarter, owner_slot):
        src, dst = pairs[arr]
        return push(
            src.at[slot], dst.at[rows_of(owner_slot), columns(quarter)],
            send_a.at[arr, slot], recv_a.at[arr, slot], {"sp": partner(me, step, sources)},
        )

    def give_ct(step, slot, quarter):
        view = rows_of(partner(me, step, sources))
        send_ct[slot] = (
            slot_weight[view] * contract(place[view], out_grad[:, columns(quarter)], 1, 0)
        ).astype(jnp.bfloat16)
        first(1, step, slot, quarter, me).start()

    def give_in(step, slot, quarter):
        view = rows_of(partner(me, step, sources))
        send_in[slot] = contract(place[view], normed[:, columns(quarter)], 1, 0).astype(
            jnp.bfloat16
        )
        first(0, step, slot, quarter, me).start()

    def give(step):
        give_ct(step, step, mine)
        give_in(step, step, mine)

    half = sources // 2
    place_z = lax.div(me * 4, sources)
    at_end = (place_z == 0) | (place_z == 3)

    def nth(index):
        return 2 + lax.rem(index + half - 2, sources - 2)

    def give_second(step):
        give_ct(step, sources - 1 + step, across)
        give_in(step, sources - 1 + step, across)

    give_ct(1, 1, mine)
    give_ct(nth(0), nth(0), mine)
    loads[1].wait()
    loop(0, tokens // 16, norm_rows)
    give_in(1, 1, mine)
    give_in(nth(0), nth(0), mine)

    loop(1, sources - 2, lambda index: give(nth(index)))
    loop(2, 4, give_second)
    give_second(1)
    own = rows_of(me)

    def own_columns(quarter):
        picked = place[own]
        rows_in[own, columns(quarter)] = contract(picked, normed[:, columns(quarter)], 1, 0).astype(
            jnp.bfloat16
        )
        rows_ct[own, columns(quarter)] = (
            slot_weight[own] * contract(picked, out_grad[:, columns(quarter)], 1, 0)
        ).astype(jnp.bfloat16)

    loop(0, 4, own_columns)

    def passed(arr, step, quarter, send, recv, target):
        view = pairs[arr][1].at[rows_of(partner(me, step, sources)), columns(quarter)]
        return push(view, view, send.at[arr, step], recv.at[arr, step], {"tp": target})

    def relay(step):
        slot = partner(me, step, sources)
        for arr in range(2):
            first(arr, step, step, mine, slot).wait_recv()
            passed(arr, step, mine, send_c, recv_c, across).start()
            passed(arr, step, mine, send_b, recv_b, beside).start()

    def onward(step):
        for arr in range(2):
            passed(arr, step, across, send_c, recv_c, across).wait_recv()
            passed(arr, step, across, send_d, recv_d, beside).start()

    def complete(step):
        for arr in range(2):
            passed(arr, step, beside, send_b, recv_b, beside).wait_recv()
            passed(arr, step, diagonal, send_d, recv_d, beside).wait_recv()

    def compute(step):
        view = rows_of(partner(me, step, sources))
        inputs = rows_in[view]
        gate_pre = contract(inputs, gate_w[...], 1, 0)
        up_pre = contract(inputs, up_w[...], 1, 0)
        logistic = jax.nn.sigmoid(gate_pre)
        gated = gate_pre * logistic
        hidden[view] = (gated * up_pre).astype(jnp.bfloat16)
        hidden_grad = contract(rows_ct[view], down_w[...], 1, 1)
        up_grad = (hidden_grad * gated).astype(jnp.bfloat16)
        gate_grad = (
            hidden_grad * up_pre * (logistic * (1.0 + gate_pre * (1.0 - logistic)))
        ).astype(jnp.bfloat16)
        pre_grad[view, :units] = gate_grad
        pre_grad[view, units:] = up_grad

        def back_columns(quarter):
            rows = columns(quarter)
            part[view, rows] = (
                contract(gate_grad, gate_w[rows], 1, 1) + contract(up_grad, up_w[rows], 1, 1)
            ).astype(jnp.bfloat16)

        loop(0, 4, back_columns)

    def part_of(step, quarter):
        return part[rows_of(partner(me, step, sources)), columns(quarter)].astype(jnp.float32)

    def near_copy(step, half, quarter):
        return push(
            part.at[rows_of(partner(me, step, sources)), columns(quarter)], near.at[step, half],
            send_n.at[step, half], recv_n.at[step, half], {"tp": beside},
        )

    def far_copy(step):
        return push(
            send_in.at[step], distant.at[step], send_f.at[step], recv_f.at[step], {"tp": across}
        )

    def home_copy(step, slot):
        return push(
            send_ct.at[step], back.at[rows_of(slot)], send_h.at[step], recv_h.at[step],
            {"sp": partner(me, step, sources)},
        )

    def share_near(step):
        near_copy(step, 1, diagonal).start()
        near_copy(step, 0, beside).start()

    def share_far(step):
        near_copy(step, 1, diagonal).wait_recv()

        @pl.when(step > 0)
        def _():
            first(0, step, step, mine, me).wait_send()

        send_in[step] = (part_of(step, across) + near[step, 1].astype(jnp.float32)).astype(
            jnp.bfloat16
        )
        far_copy(step).start()

    def send_home(step):
        near_copy(step, 0, beside).wait_recv()
        far_copy(step).wait_recv()
        total = (
            part_of(step, mine)
            + near[step, 0].astype(jnp.float32)
            + distant[step].astype(jnp.float32)
        ).astype(jnp.bfloat16)

        @pl.when(step > 0)
        def _():
            first(1, step, step, mine, me).wait_send()
            send_ct[step] = total
            home_copy(step, me).start()

        @pl.when(step == 0)
        def _():
            back[own] = total

    for copy in loads[2:]:
        copy.wait()

    def turn(index):
        early = jnp.where(at_end, sources - 2, half)
        late = jnp.where(at_end | (index < half), index, index + 2)
        step = jnp.where(index < 2, 1, jnp.where(index < 4, early + index - 2, jnp.where(index < sources - 2, late, index - sources + 4)))
        return jnp.where(index == 0, 0, step)

    def relay_turn(index):
        step = turn(index)

        @pl.when(step < 4)
        def _():
            slot = partner(me, step, sources)
            for arr in range(2):
                first(arr, step, step, mine, slot).wait_recv()
                passed(arr, step, mine, send_b, recv_b, beside).start()
            for arr in range(2):
                first(arr, step, sources - 1 + step, across, slot).wait_recv()
                passed(arr, step, across, send_d, recv_d, beside).start()

        @pl.when(step > 3)
        def _():
            relay(step)

    def onward_turn(index):
        @pl.when(turn(index) > 3)
        def _():
            onward(turn(index))

    def stage(index):
        step = turn(index)

        @pl.when(index > 0)
        def _():
            complete(step)

        compute(step)
        share_near(step)
        share_far(step)

        @pl.when(index == 0)
        def _():
            relay_turn(1)

        @pl.when(index + 2 < sources)
        def _():
            relay_turn(index + 2)

        @pl.when(index + 1 < sources)
        def _():
            onward_turn(index + 1)

        @pl.when(index > 0)
        def _():
            send_home(turn(index - 1))

    loop(0, sources, stage)
    run = model // 8

    def stored(index):
        view = pl.ds(pl.multiple_of(index * run, run), run)
        return [
            pltpu.make_async_copy(src.at[where], dst.at[where], store.at[arr, index])
            for arr, (src, dst, where) in enumerate(
                ((gate_wg, gate_out, view), (up_wg, up_out, view), (down_wg, down_out, (slice(None), view)))
            )
        ]

    def weight_run(index):
        view = pl.ds(pl.multiple_of(index * run, run), run)
        both = contract(rows_in[:, view], pre_grad[...], 0, 0).astype(jnp.bfloat16)
        gate_wg[view] = both[:, :units]
        up_wg[view] = both[:, units:]
        down_wg[:, view] = contract(hidden[...], rows_ct[:, view], 0, 0).astype(jnp.bfloat16)
        for copy in stored(index):
            copy.start()

    loop(0, 5, weight_run)
    send_home(turn(sources - 1))
    loop(5, 8, weight_run)

    def finish_home(step):
        home_copy(step, partner(me, step, sources)).wait_recv()

    loop(1, sources, finish_home)
    row_grad[...] = contract(place[...], back[...], 0, 0).astype(jnp.bfloat16)

    def finish_sends(step):
        near_copy(step, 0, beside).wait_send()
        near_copy(step, 1, diagonal).wait_send()
        far_copy(step).wait_send()

        @pl.when(step > 0)
        def _():
            home_copy(step, me).wait_send()
            for arr in range(2):
                passed(arr, step, mine, send_b, recv_b, beside).wait_send()
                passed(arr, step, across, send_d, recv_d, beside).wait_send()

        @pl.when(step > 3)
        def _():
            for arr in range(2):
                passed(arr, step, mine, send_c, recv_c, across).wait_send()

    loop(0, sources, finish_sends)
    for step in range(1, 4):
        for arr in range(2):
            first(arr, step, sources - 1 + step, across, me).wait_send()

    def finish_stores(index):
        for copy in stored(index):
            copy.wait()

    loop(0, 8, finish_stores)


def front(sources, capacity, *operands):
    stream, gate_weight, down_weight = operands[0], operands[5], operands[7]
    tokens, model = stream.shape
    units = gate_weight.shape[1]
    slots, width = sources * capacity, model // 4
    narrow = jnp.bfloat16
    vmem, anywhere = pl.BlockSpec(memory_space=pltpu.VMEM), pl.BlockSpec(memory_space=pl.ANY)
    tall, wide = gate_weight.shape, down_weight.shape
    dma = pltpu.SemaphoreType.DMA
    return pl.pallas_call(
        functools.partial(front_kernel, sources, capacity),
        out_shape=(
            jax.ShapeDtypeStruct((tokens, width), narrow),
            jax.ShapeDtypeStruct(tall, narrow),
            jax.ShapeDtypeStruct(tall, narrow),
            jax.ShapeDtypeStruct(wide, narrow),
        ),
        in_specs=[anywhere] * 2 + [vmem] * 3 + [anywhere] * 3,
        out_specs=[vmem] + [anywhere] * 3,
        scratch_shapes=[
            pltpu.VMEM((tokens, model), narrow), pltpu.VMEM((tokens, model), narrow),
            pltpu.VMEM(tall, narrow), pltpu.VMEM(tall, narrow), pltpu.VMEM(wide, narrow),
            pltpu.VMEM(tall, narrow), pltpu.VMEM(tall, narrow), pltpu.VMEM(wide, narrow),
            pltpu.VMEM((slots, tokens), narrow),
            pltpu.VMEM((slots, 1), jnp.float32),
            pltpu.VMEM((tokens, model), narrow),
            pltpu.VMEM((sources + 3, capacity, width), narrow),
            pltpu.VMEM((sources + 3, capacity, width), narrow),
            pltpu.VMEM((slots, model), narrow),
            pltpu.VMEM((slots, model), narrow),
            pltpu.VMEM((slots, model), narrow),
            pltpu.VMEM((sources, 2, capacity, width), narrow),
            pltpu.VMEM((sources, capacity, width), narrow),
            pltpu.VMEM((slots, width), narrow),
            pltpu.VMEM((slots, units), narrow),
            pltpu.VMEM((slots, 2 * units), narrow),
            dma((5,)), dma((3, 8)), dma((2, sources + 3)), dma((2, sources + 3)),
        ] + [dma((2, sources))] * 6 + [dma((sources, 2))] * 2 + [dma((sources,))] * 4,
        compiler_params=pltpu.CompilerParams(
            collective_id=0, has_side_effects=True, vmem_limit_bytes=67043328
        ),
    )(*operands)


def settle_kernel(*refs):
    count = (len(refs) - 2) // 3
    load, store = refs[-2:]
    loads = [pltpu.make_async_copy(refs[i], refs[2 * count + i], load.at[i]) for i in range(count)]
    stores = [
        pltpu.make_async_copy(refs[2 * count + i], refs[count + i], store.at[i])
        for i in range(count)
    ]
    for copy in loads:
        copy.start()
    for before, after in zip(loads, stores):
        before.wait()
        after.start()
    for copy in stores:
        copy.wait()


def settle(*arrays):
    anywhere = pl.BlockSpec(memory_space=pl.ANY)
    dma = pltpu.SemaphoreType.DMA((len(arrays),))
    return pl.pallas_call(
        settle_kernel,
        out_shape=tuple(jax.ShapeDtypeStruct(a.shape, a.dtype) for a in arrays),
        in_specs=[anywhere] * len(arrays),
        out_specs=[anywhere] * len(arrays),
        scratch_shapes=[pltpu.VMEM(a.shape, a.dtype) for a in arrays] + [dma, dma],
    )(*arrays)


def tail_kernel(
    sources, row_grad, out_hbm, stream_hbm, gain, proj_hbm, conv, branch, dmap, imap,
    dparam, dshift, states, conv_grad, branch_grad, proj_grad,
    out_grad, stream, out_proj, load, normed_grad, grad_b, rows, sums, lru, scale, gates, state_grad, reach, inner,
    send_x, recv_x, send_b, recv_b, send_d, recv_d,
    send_p, recv_p, send_px, recv_px, send_pb, recv_pb, send_pd, recv_pd, send_s, recv_s,
    send_l, recv_l
):
    me, mine = lax.axis_index("sp"), lax.axis_index("tp")
    beside = mine + 1 - 2 * lax.rem(mine, 2)
    across = lax.rem(mine + 2, 4)
    diagonal = lax.rem(beside + 2, 4)
    tokens, width = out_grad.shape
    quarter = width // 4
    chunk = tokens // 4
    piece = width // sources
    channels = conv.shape[1]
    announce(sources, me, (beside, across))
    loads = [
        pltpu.make_async_copy(src, dst, load.at[index])
        for index, (src, dst) in enumerate(
            ((stream_hbm, stream), (out_hbm, out_grad), (proj_hbm, out_proj))
        )
    ]
    for copy in loads:
        copy.start()
    normed_grad[mine] = row_grad[...]
    gate = branch[...].astype(jnp.float32)
    slope = 0.7978845608028654
    inside = jnp.tanh(slope * (gate + 0.044715 * gate * gate * gate))
    lru[me] = ((states[0] + states[1]) * (0.5 * gate * (1.0 + inside))).astype(jnp.bfloat16)
    all_here(sources, (beside, across))

    def part(which, index, send, recv, target):
        view = normed_grad.at[which, pl.ds(index * chunk, chunk)]
        return push(view, view, send.at[index], recv.at[index], {"tp": target})

    for index in range(4):
        part(mine, index, send_x, recv_x, across).start()
        part(mine, index, send_b, recv_b, beside).start()

    def lru_copy(step, slot):
        return push(
            lru.at[slot], lru.at[slot], send_l.at[step], recv_l.at[step],
            {"sp": partner(me, step, sources)},
        )

    half = sources // 2
    early = half + (3 * half) // 4
    lru_copy(1, me).start()
    loop(half, early, lambda step: lru_copy(step, me).start())

    def squares(index):
        low = pl.multiple_of(index * 16, 16)
        total = jnp.zeros((16, 1), jnp.float32)
        for q in range(4):
            values = stream[pl.ds(low, 16), q * quarter : (q + 1) * quarter].astype(jnp.float32)
            total = total + jnp.sum(values * values, axis=1, keepdims=True)
        scale[pl.ds(low, 16)] = lax.rsqrt(total / width + norm_eps)

    loads[0].wait()
    loop(0, tokens // 16, squares)
    loads[1].wait()
    loads[2].wait()

    def relay_part(index):
        part(across, index, send_x, recv_x, across).wait_recv()
        part(across, index, send_d, recv_d, beside).start()

    block = 64
    for direction in range(2):
        relay_part(2 * direction)
        base = softplus(-dparam[direction : direction + 1])
        def gate_rows(index):
            low = pl.multiple_of(index * block, block)
            view = pl.ds(low, block)
            held = conv[view]
            decay_gate = jax.nn.sigmoid(contract(held, dmap[direction], 1, 0))
            input_gate = jax.nn.sigmoid(contract(held, imap[direction], 1, 0))
            log_decay = -rate_scale * decay_gate * base + dshift[direction, view]
            gates[4 * direction, view] = decay_gate
            gates[4 * direction + 1, view] = input_gate
            gates[4 * direction + 2, view] = jnp.exp(log_decay)
            gates[4 * direction + 3, view] = jnp.sqrt(minus_expm1(2.0 * log_decay))
        loop(0, tokens // block, gate_rows)
        relay_part(2 * direction + 1)

    def piece_copy(step):
        peer = partner(me, step, sources)
        return push(
            grad_b.at[pl.ds(pl.multiple_of(mine * chunk, chunk), chunk), pl.ds(pl.multiple_of(peer * piece, piece), piece)],
            rows.at[me, pl.ds(pl.multiple_of(mine * chunk, chunk), chunk)],
            send_p.at[step], recv_p.at[step], {"sp": peer},
        )

    def piece_landed(step):
        peer = partner(me, step, sources)
        return push(
            grad_b.at[pl.ds(pl.multiple_of(mine * chunk, chunk), chunk), pl.ds(pl.multiple_of(me * piece, piece), piece)],
            rows.at[peer, pl.ds(pl.multiple_of(mine * chunk, chunk), chunk)],
            send_p.at[step], recv_p.at[step], {"sp": peer},
        )

    def piece_pass(step, which, send, recv, target):
        view = rows.at[partner(me, step, sources), pl.ds(pl.multiple_of(which * chunk, chunk), chunk)]
        return push(view, view, send.at[step], recv.at[step], {"tp": target})

    for index in range(4):
        part(beside, index, send_b, recv_b, beside).wait_recv()
        part(diagonal, index, send_d, recv_d, beside).wait_recv()

        def grad_rows(inside):
            low = pl.multiple_of(index * chunk + inside * 16, 16)
            view = pl.ds(low, 16)
            own_scale = scale[view]
            total = jnp.zeros((16, 1), jnp.float32)
            for q in range(4):
                run = slice(q * quarter, (q + 1) * quarter)
                scaled = gain[run].astype(jnp.float32)[None, :] * normed_grad[q, view].astype(jnp.float32)
                total = total + jnp.sum(
                    stream[view, run].astype(jnp.float32) * scaled, axis=1, keepdims=True
                )
            factor = own_scale * own_scale * total / width
            for q in range(4):
                run = slice(q * quarter, (q + 1) * quarter)
                scaled = gain[run].astype(jnp.float32)[None, :] * normed_grad[q, view].astype(jnp.float32)
                grad_b[view, run] = (
                    out_grad[view, run].astype(jnp.float32)
                    + own_scale * (scaled - stream[view, run].astype(jnp.float32) * factor)
                ).astype(jnp.bfloat16)

        loop(0, chunk // 16, grad_rows)

        @pl.when(mine == index)
        def _():
            loop(1, sources, lambda step: piece_copy(sources - step).start())

    lru_out_grad = contract(grad_b[...], out_proj[...], 1, 0)
    gate = branch[...].astype(jnp.float32)
    slope = 0.7978845608028654
    inside = jnp.tanh(slope * (gate + 0.044715 * gate * gate * gate))
    gelu_gate = 0.5 * gate * (1.0 + inside)
    gelu_slope = 0.5 * (1.0 + inside) + 0.5 * gate * (1.0 - inside * inside) * slope * (
        1.0 + 3.0 * 0.044715 * gate * gate
    )
    branch_grad[...] = lru_out_grad * (states[0] + states[1]) * gelu_slope
    state_grad[...] = lru_out_grad * gelu_gate

    def relay(step):
        piece_landed(step).wait_recv()
        piece_pass(step, mine, send_px, recv_px, across).start()
        piece_pass(step, mine, send_pb, recv_pb, beside).start()

    def onward(step):
        piece_pass(step, across, send_px, recv_px, across).wait_recv()
        piece_pass(step, across, send_pd, recv_pd, beside).start()

    place = lax.broadcasted_iota(jnp.int32, (tokens, channels), 0)
    for direction in range(2):
        decay = gates[4 * direction + 2]
        if direction == 0:
            coeffs = jnp.where(place < tokens - 1, pltpu.roll(decay, tokens - 1, 0), 1.0)
            edge = 0
        else:
            coeffs = jnp.where(place >= 1, pltpu.roll(decay, 1, 0), 1.0)
            edge = tokens - 1
        coeffs, values = scan_rows(coeffs, state_grad[...], direction == 0)
        reach[direction] = coeffs
        inner[direction] = values
        edge_decay = decay[edge : edge + 1]
        sums[me, 2 * direction : 2 * direction + 1] = edge_decay * coeffs[edge : edge + 1]
        sums[me, 2 * direction + 1 : 2 * direction + 2] = edge_decay * values[edge : edge + 1]

    def sums_copy(step, slot):
        return push(
            sums.at[slot], sums.at[slot], send_s.at[step], recv_s.at[step],
            {"sp": partner(me, step, sources)},
        )

    loop(1, sources, lambda step: sums_copy(sources - step, me).start())
    loop(early, sources, lambda step: lru_copy(step, me).start())
    loop(2, half, lambda step: lru_copy(step, me).start())
    loop(1, half, relay)
    loop(1, half, onward)
    loop(half, sources, relay)
    loop(1, sources, lambda step: sums_copy(step, partner(me, step, sources)).wait_recv())
    zero_row = jnp.zeros((1, channels), jnp.float32)

    def from_right(index, carry):
        slot = sources - 1 - index
        ours = sums[slot, 0:1] * carry + sums[slot, 1:2]
        return jnp.where(slot > me, ours, carry)

    def from_left(slot, carry):
        ours = sums[slot, 2:3] * carry + sums[slot, 3:4]
        return jnp.where(slot < me, ours, carry)

    incoming = (
        lax.fori_loop(0, sources, from_right, zero_row),
        lax.fori_loop(0, sources, from_left, zero_row),
    )
    for direction in range(2):
        base = softplus(-dparam[direction : direction + 1])

        def back_rows(index):
            view = pl.ds(pl.multiple_of(index * block, block), block)
            decay_gate, input_gate = gates[4 * direction, view], gates[4 * direction + 1, view]
            decay_rate, drive_scale = gates[4 * direction + 2, view], gates[4 * direction + 3, view]
            conv_float = conv[view].astype(jnp.float32)
            adjoint = inner[direction, view] + reach[direction, view] * incoming[direction]
            driven = input_gate * conv_float
            log_grad = adjoint * (
                states[direction, view] - drive_scale * driven
                - driven * decay_rate * decay_rate / drive_scale
            )
            decay_pre_grad = log_grad * (-rate_scale * base) * decay_gate * (1.0 - decay_gate)
            input_pre_grad = adjoint * drive_scale * driven * (1.0 - input_gate)
            ours = (
                adjoint * drive_scale * input_gate
                + split_dot(decay_pre_grad, dmap[direction])
                + split_dot(input_pre_grad, imap[direction])
            )
            conv_grad[view] = ours if direction == 0 else conv_grad[view] + ours

        loop(0, tokens // block, back_rows)
    loop(half, sources, onward)
    proj_grad[...] = contract(
        grad_b[:, pl.ds(pl.multiple_of(me * piece, piece), piece)], lru[me], 0, 0
    )

    def gather_product(step):
        slot = partner(me, step, sources)
        lru_copy(step, slot).wait_recv()
        piece_pass(step, beside, send_pb, recv_pb, beside).wait_recv()
        piece_pass(step, diagonal, send_pd, recv_pd, beside).wait_recv()
        proj_grad[...] += contract(rows[slot], lru[slot], 0, 0)

    loop(1, sources, gather_product)

    def finish(step):
        piece_copy(step).wait_send()
        piece_pass(step, mine, send_px, recv_px, across).wait_send()
        piece_pass(step, mine, send_pb, recv_pb, beside).wait_send()
        piece_pass(step, across, send_pd, recv_pd, beside).wait_send()
        sums_copy(step, me).wait_send()
        lru_copy(step, me).wait_send()

    loop(1, sources, finish)
    for index in range(4):
        part(mine, index, send_x, recv_x, across).wait_send()
        part(mine, index, send_b, recv_b, beside).wait_send()
        part(across, index, send_d, recv_d, beside).wait_send()


def tail(sources, *operands):
    out_grad, conv = operands[1], operands[5]
    tokens, width = out_grad.shape
    channels = conv.shape[1]
    plane = (tokens, channels)
    four = pltpu.SemaphoreType.DMA((4,))
    each = pltpu.SemaphoreType.DMA((sources,))
    return pl.pallas_call(
        functools.partial(tail_kernel, sources),
        out_shape=(
            jax.ShapeDtypeStruct(plane, jnp.float32),
            jax.ShapeDtypeStruct(plane, jnp.float32),
            jax.ShapeDtypeStruct((width // sources, channels), jnp.float32),
        ),
        in_specs=[
            pl.BlockSpec(memory_space=pl.ANY if index in (1, 2, 4) else pltpu.VMEM)
            for index in range(len(operands))
        ],
        out_specs=[pl.BlockSpec(memory_space=pltpu.VMEM)] * 3,
        scratch_shapes=[
            pltpu.VMEM((tokens, width), jnp.bfloat16),
            pltpu.VMEM((tokens, width), jnp.bfloat16),
            pltpu.VMEM((width, channels), jnp.bfloat16),
            pltpu.SemaphoreType.DMA((3,)),
            pltpu.VMEM((4, tokens, width // 4), jnp.bfloat16),
            pltpu.VMEM((tokens, width), jnp.bfloat16),
            pltpu.VMEM((sources, tokens, width // sources), jnp.bfloat16),
            pltpu.VMEM((sources, 8, channels), jnp.float32),
            pltpu.VMEM((sources, tokens, channels), jnp.bfloat16),
            pltpu.VMEM((tokens, 1), jnp.float32),
            pltpu.VMEM((8,) + plane, jnp.float32),
            pltpu.VMEM(plane, jnp.float32),
            pltpu.VMEM((2,) + plane, jnp.float32),
            pltpu.VMEM((2,) + plane, jnp.float32),
        ] + [four] * 6 + [each] * 12,
        compiler_params=pltpu.CompilerParams(collective_id=1, has_side_effects=True),
    )(*operands)


def body(
    out_grad,
    stream,
    norm_gain,
    routes,
    route_weight,
    gate_weight,
    up_weight,
    down_weight,
    out_proj,
    conv_out,
    gate_branch,
    decay_map,
    input_map,
    decay_param,
    decay_shift,
    states,
):
    sources = lax.axis_size("sp")
    experts = EXP_DEV * sources
    capacity = (5 * TOP * TOK_DEV + 4 * experts - 1) // (4 * experts)
    capacity = (capacity + 15) // 16 * 16
    row_grad, gate_grads, up_grads, down_grads = front(
        sources,
        capacity,
        stream,
        out_grad,
        norm_gain,
        routes.T,
        route_weight.T,
        gate_weight[0],
        up_weight[0],
        down_weight[0],
    )
    conv_grad, gate_branch_grad, out_proj_grad = tail(
        sources,
        row_grad,
        out_grad,
        stream,
        norm_gain,
        out_proj,
        conv_out,
        gate_branch,
        decay_map[:, 0],
        input_map[:, 0],
        decay_param,
        decay_shift,
        states,
    )
    gate_grads, up_grads, down_grads, conv_grad, gate_branch_grad, out_proj_grad = settle(
        gate_grads, up_grads, down_grads, conv_grad, gate_branch_grad, out_proj_grad
    )
    return (
        conv_grad,
        gate_branch_grad,
        out_proj_grad,
        gate_grads[None],
        up_grads[None],
        down_grads[None],
    )


def solution(mesh):
    placed = (
        P("sp", None),
        P("sp", None),
        P(),
        P("sp", None),
        P("sp", None),
        P("sp", None, "tp"),
        P("sp", None, "tp"),
        P("sp", "tp", None),
        P(None, "tp"),
        P("sp", "tp"),
        P("sp", "tp"),
        P(None, "tp", None, None),
        P(None, "tp", None, None),
        P(None, "tp"),
        P(None, "sp", "tp"),
        P(None, "sp", "tp"),
    )
    return jax.shard_map(
        body,
        mesh=mesh,
        in_specs=placed,
        out_specs=(
            P("sp", "tp"),
            P("sp", "tp"),
            P("sp", "tp"),
            P("sp", None, "tp"),
            P("sp", None, "tp"),
            P("sp", "tp", None),
        ),
        check_vma=False,
    )
```
